128 devices in a mesh: kv: 32 (over z, y, core), tp: 4 (over x).
Axes of the slice: x: 4, y: 4, z: 4, core: 2. Of those that a mesh axis runs over, the one named last changes fastest.
Arguments:
- layer_input: bfloat16 [4, 16384, 2048], P(None, 'kv', 'tp'), may hold values from -0.119628906 to 0.119628906
- queries: bfloat16 [4, 16384, 2048], P(None, 'kv', 'tp'), may hold values from -3.5 to 3.5
- keys: bfloat16 [4, 16384, 2048], P(None, 'kv', 'tp'), may hold values from -3.5 to 3.5
- values: bfloat16 [4, 16384, 2048], P(None, 'kv', 'tp'), may hold values from -5 to 5
- outputs: bfloat16 [4, 16384, 2048], P(None, 'kv', 'tp'), may hold values from -1.5 to 1.5
- d_out: bfloat16 [4, 16384, 2048], P(None, 'kv', 'tp'), may hold values from -30 to 30
- log_sums: float32 [4, 16384, 16], P(None, 'kv', 'tp'), may hold values from 6 to 8
- chosen: int32 [4, 256, 12], P(None, 'kv'), may hold values from -1 to 255, as said below
Outputs:
- d_queries: bfloat16 [4, 16384, 2048], P(None, 'kv', 'tp')
- d_keys: bfloat16 [4, 16384, 2048], P(None, 'kv', 'tp')
- d_values: bfloat16 [4, 16384, 2048], P(None, 'kv', 'tp')
- d_weight: float32 [2048, 2048], P('kv', 'tp')
The draws below stay inside these ranges and needn't reach their ends.
Inputs may be any that keep to these rules, and one draw needn't show every extreme that they name: Row chosen[s, b] names key blocks of sequence s for query block b: its first entry is b itself, the others are distinct blocks with smaller indices, either on the same device as b or on earlier devices; -1 marks unused slots, which come last. Over all sequences, the blocks of one device that query blocks of other devices name are at most 2, and in every draw some devices' are exactly 2.
All inputs are finite; a program needn't handle non-finite values.
Results may differ from the reference program's by a relative error of at most 0.0055.
Values may be sent and summed in bfloat16 or wider, within the bound.
A program may use at most 256 MiB of HBM per device.

```python
import jax
import jax.numpy as jnp
from jax import lax

D = 2048
HEADS = 16
DH = 128
HD = 2048
BLK = 64
SEL = 12
CAP = 2
SEQS = 4
TOK_DEV = 512
NPOS = 16384
NBLK = 256


def draw_chosen(key, part):
    local_blocks = TOK_DEV // BLK
    devices = NBLK // local_blocks
    own_blocks = SEQS * local_blocks
    pool_size = local_blocks + devices * CAP
    publish_key = jax.random.fold_in(key, 11)
    choose_key = jax.random.fold_in(key, 12)
    ranking = jax.random.randint(publish_key, (devices, own_blocks), 0, 4096) * own_blocks
    ranking = ranking + jnp.arange(own_blocks, dtype=jnp.int32)[None, :]
    published = jnp.argsort(-ranking, axis=1)[:, :CAP].astype(jnp.int32)
    owner_ids = jnp.arange(devices, dtype=jnp.int32)
    remote_seq = (published // local_blocks).reshape(devices * CAP)
    remote_block = (owner_ids[:, None] * local_blocks + published % local_blocks).reshape(devices * CAP)
    remote_owner = jnp.repeat(owner_ids, CAP)
    sequence_ids = jnp.arange(SEQS, dtype=jnp.int32)[:, None, None]
    query_block = jnp.arange(NBLK, dtype=jnp.int32)[None, :, None]
    query_device = query_block // local_blocks
    query_local = query_block % local_blocks
    local_index = jnp.arange(local_blocks, dtype=jnp.int32)[None, None, :]
    local_extent = (SEQS, NBLK, local_blocks)
    remote_extent = (SEQS, NBLK, devices * CAP)
    local_block = jnp.broadcast_to(query_device * local_blocks + local_index, local_extent)
    local_ok = jnp.broadcast_to(local_index <= query_local, local_extent)
    local_level = jnp.broadcast_to((local_index == query_local).astype(jnp.int32) * 4, local_extent)
    remote_ok = (remote_owner[None, None, :] < query_device) & (remote_seq[None, None, :] == sequence_ids)
    nearby = (remote_owner[None, None, :] == query_device - 1) | (remote_owner[None, None, :] == query_device - devices // 2)
    remote_level = jnp.broadcast_to(nearby.astype(jnp.int32) * 2, remote_extent)
    blocks = jnp.concatenate([local_block, jnp.broadcast_to(remote_block[None, None, :], remote_extent)], axis=2)
    usable = jnp.concatenate([local_ok, jnp.broadcast_to(remote_ok, remote_extent)], axis=2)
    levels = jnp.concatenate([local_level, remote_level], axis=2)
    slot_ids = jnp.arange(pool_size, dtype=jnp.int32)
    jitter = jax.random.randint(choose_key, (SEQS, NBLK, pool_size), 0, 4096)
    scores = (levels * 4096 + jitter) * pool_size + slot_ids
    scores = jnp.where(usable, scores, -1 - slot_ids)
    ranked = jnp.argsort(-scores, axis=2)[:, :, :SEL]
    top_scores = jnp.take_along_axis(scores, ranked, axis=2)
    picked = jnp.take_along_axis(blocks, ranked, axis=2)
    return jnp.where(top_scores >= 0, picked, -1).astype(jnp.int32)


def spiked(values, key, source, target, shards_of, factor):
    owner, partner = [(jnp.arange(values.shape[axis_at]) // (values.shape[axis_at] // shards_of)).reshape([-1 if axis == axis_at else 1 for axis in range(values.ndim)]) for axis_at in (source, target)]
    chosen = jax.random.permutation(key, shards_of)[partner]
    strong = (owner == chosen) | (owner == (partner + shards_of // 2) % shards_of)
    return jnp.where(strong, factor * values, values)


def block_scale(stream_key, shape, shards, smallest, largest):
    gain, own = 1.0, jax.random.fold_in(stream_key, 6)
    for position, blocks in shards:
        draws = jnp.exp(jax.random.uniform(jax.random.fold_in(own, position), (blocks,), jnp.float32, smallest / len(shards), largest / len(shards)))
        gain = gain * jnp.repeat(draws, shape[position] // blocks).reshape([-1 if axis == position else 1 for axis in range(len(shape))])
    return gain


def normal_values(own_key, shape, scale, reach, shards=(), kind=jnp.bfloat16):
    array = scale * jax.random.normal(own_key, shape, jnp.float32)
    if shards:
        array = array * block_scale(own_key, shape, shards, -0.22, 0.18)
    return jnp.clip(array, -reach, reach).astype(kind)


def bell_draw_with(stream_key, shape, width, reach, cuts, heavy, kind=jnp.bfloat16):
    result = width * jax.random.normal(stream_key, shape, jnp.float32)
    if cuts:
        result = result * block_scale(stream_key, shape, cuts, -0.22, 0.18)
    return jnp.clip(spiked(result, jax.random.fold_in(stream_key, 3), *heavy), -reach, reach).astype(kind)


def setup_inputs(seed: int = 0) -> dict:
    seeds = jax.random.split(jax.random.key(seed), 9)
    layer_input = bell_draw_with(seeds[0], (SEQS, NPOS, D), 0.02, 0.119628906, ((1, 32), (2, 4)), (1, 2, 32, 2.75))
    queries = normal_values(seeds[1], (SEQS, NPOS, HD), 0.7, 3.5, ((1, 32), (2, 4)))
    keys = normal_values(seeds[2], (SEQS, NPOS, HD), 0.7, 3.5, ((1, 32), (2, 4)))
    values = normal_values(seeds[3], (SEQS, NPOS, HD), 1.0, 5.0, ((1, 32), (2, 4)))
    outputs = normal_values(seeds[4], (SEQS, NPOS, HD), 0.25, 1.5, ((1, 32), (2, 4)))
    d_out = normal_values(seeds[5], (SEQS, NPOS, HD), 6.0, 30.0, ((1, 32), (2, 4)))
    log_sums = jnp.clip(6.0 + 2.0 * jax.random.uniform(seeds[6], (SEQS, NPOS, HEADS), jnp.float32) ** block_scale(seeds[6], (SEQS, NPOS, HEADS), ((1, 32), (2, 4)), -0.2, 0.2), 6.0, 8.0)
    chosen = draw_chosen(jax.random.fold_in(seeds[8], 71), 0)
    return dict(layer_input=layer_input, queries=queries, keys=keys, values=values, outputs=outputs, d_out=d_out, log_sums=log_sums, chosen=chosen)


def one_sequence(bundle):
    queries, keys, values, outputs, d_out, log_sums, chosen = bundle
    inverse_root = DH ** -0.5
    query_blocks = queries.reshape(NBLK, BLK, HEADS, DH)
    key_blocks = keys.reshape(NBLK, BLK, HEADS, DH)
    value_blocks = values.reshape(NBLK, BLK, HEADS, DH)
    cotangent = d_out.reshape(NBLK, BLK, HEADS, DH)
    product = d_out.astype(jnp.float32) * outputs.astype(jnp.float32)
    deltas = jnp.sum(product.reshape(NBLK, BLK, HEADS, DH), axis=3)
    log_blocks = log_sums.reshape(NBLK, BLK, HEADS)
    offsets = jnp.arange(BLK, dtype=jnp.int32)

    def advance(totals, block_index):
        key_total, value_total = totals
        picked = chosen[block_index]
        in_use = picked >= 0
        clamped = jnp.maximum(picked, 0).astype(jnp.int32)
        key_picked = key_blocks[clamped].astype(jnp.float32)
        value_picked = value_blocks[clamped].astype(jnp.float32)
        key_place = clamped[:, None] * BLK + offsets[None, :]
        query_place = block_index * BLK + offsets
        visible = in_use[None, :, None] & (key_place[None, :, :] <= query_place[:, None, None])
        query_rows = query_blocks[block_index].astype(jnp.float32)
        grad_rows = cotangent[block_index].astype(jnp.float32)
        scores = jnp.einsum('qhd,ekhd->hqek', query_rows, key_picked) * inverse_root
        log_shift = log_blocks[block_index].T[:, :, None, None]
        prob_full = jnp.where(visible[None], jnp.exp(scores - log_shift), 0.0)
        prob_grad = jnp.einsum('qhd,ekhd->hqek', grad_rows, value_picked)
        score_grad = prob_full * (prob_grad - deltas[block_index].T[:, :, None, None])
        prob_low = lax.optimization_barrier(prob_full.astype(jnp.bfloat16)).astype(jnp.float32)
        score_low = lax.optimization_barrier(score_grad.astype(jnp.bfloat16)).astype(jnp.float32)
        grad_query = jnp.einsum('hqek,ekhd->qhd', score_low, key_picked) * inverse_root
        grad_key = jnp.einsum('hqek,qhd->ekhd', score_low, query_rows) * inverse_root
        grad_value = jnp.einsum('hqek,qhd->ekhd', prob_low, grad_rows)
        weight = in_use.astype(jnp.float32)[:, None, None, None]
        key_total = key_total.at[clamped].add(grad_key * weight)
        value_total = value_total.at[clamped].add(grad_value * weight)
        return (key_total, value_total), grad_query.astype(jnp.bfloat16)

    zeroed = jnp.zeros((NBLK, BLK, HEADS, DH), jnp.float32)
    totals, grad_query = lax.scan(advance, (zeroed, zeroed), jnp.arange(NBLK, dtype=jnp.int32))
    key_total, value_total = totals
    d_queries = grad_query.reshape(NPOS, HEADS * DH)
    d_keys = key_total.astype(jnp.bfloat16).reshape(NPOS, HEADS * DH)
    d_values = value_total.astype(jnp.bfloat16).reshape(NPOS, HEADS * DH)
    return d_queries, d_keys, d_values


def reference(layer_input, queries, keys, values, outputs, d_out, log_sums, chosen):
    d_queries, d_keys, d_values = lax.map(one_sequence, (queries, keys, values, outputs, d_out, log_sums, chosen))
    flat_input = layer_input.reshape(SEQS * NPOS, D)
    flat_values = d_values.reshape(SEQS * NPOS, HEADS * DH)
    d_weight = jnp.dot(flat_input.T, flat_values, preferred_element_type=jnp.float32)
    return d_queries, d_keys, d_values, d_weight
```

```python
import functools
import jax
import jax.numpy as jnp
from jax import lax
from jax.experimental import pallas as pl
from jax.experimental.pallas import tpu as pltpu
from jax.sharding import PartitionSpec as P

BLK = 64
CAP = 2
DH = 128
LOG2E = 1.4426950408889634
ROOT = DH ** -0.5
BIG = 1e30

NT = (((1,), (1,)), ((), ()))
TN = (((0,), (0,)), ((), ()))
NN = (((1,), (0,)), ((), ()))


def mm(a, b, dims):
    return lax.dot_general(a, b, dims, preferred_element_type=jnp.float32)


def local_kernel(q_ref, k_ref, v_ref, o_ref, do_ref, lse_ref, sel_ref,
                 dqt_ref, dk_ref, dv_ref, delta_ref):
    heads = q_ref.shape[2] // DH
    n = q_ref.shape[1]
    half = n // 2
    for h in range(heads):
        hs = slice(h * DH, (h + 1) * DH)
        q = q_ref[0, :, hs]
        do = do_ref[0, :, hs]
        prod = do.astype(jnp.float32) * o_ref[0, :, hs].astype(jnp.float32)
        delta = jnp.sum(prod.T, axis=0, keepdims=True)
        delta_ref[0, h:h + 1, :] = delta
        lse = lse_ref[0, h:h + 1, :]
        parts = []
        for c in range(2):
            lo = c * half
            k = k_ref[0, lo:lo + half, hs]
            v = v_ref[0, lo:lo + half, hs]
            qc = q[lo:]
            doc = do[lo:]
            w = n - lo
            s = mm(k, qc, NT)
            row = lax.broadcasted_iota(jnp.int32, (half, w), 0)
            col = lax.broadcasted_iota(jnp.int32, (half, w), 1)
            bias = jnp.concatenate(
                [jnp.broadcast_to(lse[:, lo:] + sel_ref[0, j:j + 1, lo:], (BLK, w))
                 for j in range(lo // BLK, (lo + half) // BLK)], axis=0)
            x = jnp.where(row <= col, s * (ROOT * LOG2E) - bias, -BIG)
            p = jnp.exp2(x)
            dp = mm(v, doc, NT)
            ds = (p * (dp - delta[:, lo:])).astype(jnp.bfloat16)
            dv_ref[0, lo:lo + half, hs] = mm(p.astype(jnp.bfloat16), doc, NN).astype(jnp.bfloat16)
            dk_ref[0, lo:lo + half, hs] = (mm(ds, qc, NN) * ROOT).astype(jnp.bfloat16)
            parts.append(mm(k, ds, TN))
        dqt_ref[0, hs, :half] = parts[0][:, :half]
        dqt_ref[0, hs, half:] = parts[0][:, half:] + parts[1]


def remote_kernel(seq_ref, q_ref, do_ref, lse_ref, delta_ref, sel_ref, pk_ref, pv_ref, dqt_in,
                  dq_ref, gk_ref, gv_ref, acc, list_ref, cnt_ref):
    seqs = 4
    heads = q_ref.shape[2] // DH
    slots = pk_ref.shape[0]
    s = pl.program_id(0)

    @pl.when(s == 0)
    def _():
        for t in range(seqs):
            cnt_ref[t] = 0

        def scan(i, _):
            t = seq_ref[i]

            @pl.when(t >= 0)
            def _():
                c = cnt_ref[t]
                list_ref[t, c] = i
                cnt_ref[t] = c + 1

            @pl.when(t < 0)
            def _():
                gk_ref[i] = jnp.zeros(gk_ref.shape[1:], gk_ref.dtype)
                gv_ref[i] = jnp.zeros(gv_ref.shape[1:], gv_ref.dtype)
            return 0

        lax.fori_loop(0, slots, scan, 0)

    acc[...] = dqt_in[0]
    n = cnt_ref[s]

    def chunk(c, _):
        ids = []
        for e in range(4):
            at = c * 4 + e
            i = list_ref[s, jnp.minimum(at, n - 1)]
            ids.append((i, jnp.where(at < n, i, slots)))
        for h in range(heads):
            hs = slice(h * DH, (h + 1) * DH)
            q = q_ref[0, :, hs]
            do = do_ref[0, :, hs]
            k = jnp.concatenate([pk_ref[i, :, hs] for i, _ in ids], axis=0)
            v = jnp.concatenate([pv_ref[i, :, hs] for i, _ in ids], axis=0)
            lse = lse_ref[0, h:h + 1, :]
            st = mm(k, q, NT)
            bias = jnp.concatenate(
                [jnp.broadcast_to(lse + sel_ref[j], (BLK, lse.shape[1])) for _, j in ids], axis=0)
            p = jnp.exp2(st * (ROOT * LOG2E) - bias)
            dp = mm(v, do, NT)
            ds = (p * (dp - delta_ref[0, h:h + 1, :])).astype(jnp.bfloat16)
            dv = mm(p.astype(jnp.bfloat16), do, NN).astype(jnp.bfloat16)
            dk = (mm(ds, q, NN) * ROOT).astype(jnp.bfloat16)
            for e, (_, j) in enumerate(ids):
                gv_ref[j, :, hs] = dv[e * BLK:(e + 1) * BLK]
                gk_ref[j, :, hs] = dk[e * BLK:(e + 1) * BLK]
            acc[hs, :] += mm(k, ds, TN)
        return 0

    lax.fori_loop(0, (n + 3) // 4, chunk, 0)
    for h in range(heads):
        hs = slice(h * DH, (h + 1) * DH)
        dq_ref[0, :, hs] = (acc[hs, :].T * ROOT).astype(jnp.bfloat16)


def local_attention(q, k, v, o, do, lse, sel):
    seqs, n, ch = q.shape
    heads = ch // DH
    big = pl.BlockSpec((1, n, ch), lambda s: (s, 0, 0))
    small = pl.BlockSpec((1, heads, n), lambda s: (s, 0, 0))
    return pl.pallas_call(
        local_kernel,
        grid=(seqs,),
        in_specs=[big] * 5 + [small, pl.BlockSpec((1, n // BLK, n), lambda s: (s, 0, 0))],
        out_specs=[pl.BlockSpec((1, ch, n), lambda s: (s, 0, 0)), big, big, small],
        out_shape=[
            jax.ShapeDtypeStruct((seqs, ch, n), jnp.float32),
            jax.ShapeDtypeStruct(q.shape, jnp.bfloat16),
            jax.ShapeDtypeStruct(q.shape, jnp.bfloat16),
            jax.ShapeDtypeStruct((seqs, heads, n), jnp.float32),
        ],
        compiler_params=pltpu.CompilerParams(vmem_limit_bytes=48 * 1024 * 1024),
        cost_estimate=pl.CostEstimate(flops=5 * 2 * seqs * heads * n * n * DH, bytes_accessed=22 << 20,
                                      transcendentals=seqs * heads * n * n),
        name="local_attention",
    )(q, k, v, o, do, lse, sel)


def remote_attention(slot_seq, q, do, lse, delta, sel, pk, pv, dqt):
    seqs, n, ch = q.shape
    heads = ch // DH
    slots = pk.shape[0]
    big = pl.BlockSpec((1, n, ch), lambda s: (s, 0, 0))
    small = pl.BlockSpec((1, heads, n), lambda s: (s, 0, 0))
    whole = pl.BlockSpec(memory_space=pltpu.VMEM)
    return pl.pallas_call(
        remote_kernel,
        grid=(seqs,),
        in_specs=[pl.BlockSpec(memory_space=pltpu.SMEM), big, big, small, small, whole, whole, whole,
                  pl.BlockSpec((1, ch, n), lambda s: (s, 0, 0))],
        out_specs=[big, whole, whole],
        out_shape=[
            jax.ShapeDtypeStruct(q.shape, jnp.bfloat16),
            jax.ShapeDtypeStruct((slots + 1, BLK, ch), jnp.bfloat16),
            jax.ShapeDtypeStruct((slots + 1, BLK, ch), jnp.bfloat16),
        ],
        scratch_shapes=[
            pltpu.VMEM((ch, n), jnp.float32),
            pltpu.SMEM((seqs, slots), jnp.int32),
            pltpu.SMEM((seqs,), jnp.int32),
        ],
        compiler_params=pltpu.CompilerParams(vmem_limit_bytes=60 * 1024 * 1024),
        cost_estimate=pl.CostEstimate(flops=5 * 2 * heads * slots * BLK * n * DH, bytes_accessed=28 << 20,
                                      transcendentals=heads * slots * BLK * n),
        name="remote_attention",
    )(slot_seq, q, do, lse, delta, sel, pk, pv, dqt)


def first_slots(needed, slots):
    running = jnp.cumsum(needed, axis=1) - 1
    levels = jnp.arange(slots, dtype=jnp.int32)[None, :, None]
    matches = (needed[:, None, :] == 1) & (running[:, None, :] == levels)
    places = jnp.arange(needed.shape[1], dtype=jnp.int32)[None, None, :]
    present = jnp.sum(matches.astype(jnp.int32), axis=2)
    located = jnp.sum(jnp.where(matches, places, 0), axis=2)
    return jnp.where(present > 0, located, -1)


def body(layer_input, queries, keys, values, outputs, d_out, log_sums, chosen):
    seqs, n, ch = queries.shape
    local_blocks = n // BLK
    devices = lax.axis_size("kv")
    me = lax.axis_index("kv")
    own = seqs * local_blocks
    lse = jnp.swapaxes(log_sums, 1, 2) * LOG2E

    in_use = chosen >= 0
    remote = in_use & (chosen // local_blocks != me)
    ids = jnp.arange(devices * local_blocks, dtype=jnp.int32)
    needed = jnp.max(((chosen[..., None] == ids) & remote[..., None]).astype(jnp.int32), axis=(1, 2))
    needed = needed.reshape(seqs, devices, local_blocks).transpose(1, 0, 2).reshape(devices, own)
    everyone = lax.all_gather(needed, "kv").max(axis=0)
    table = first_slots(everyone, CAP)
    served = lax.dynamic_slice_in_dim(table, me, 1, 0).reshape(CAP)
    rows = jnp.maximum(served, 0)
    sent = jnp.concatenate([keys.reshape(own, BLK, ch)[rows], values.reshape(own, BLK, ch)[rows]], axis=0)
    pool = lax.all_gather(sent, "kv", axis=0)
    pk = pool[:, :CAP].reshape(devices * CAP, BLK, ch)
    pv = pool[:, CAP:].reshape(devices * CAP, BLK, ch)

    mine = me * local_blocks + jnp.arange(local_blocks, dtype=jnp.int32)
    picked = jnp.any(chosen[:, None, :, :] == mine[None, :, None, None], axis=3)
    sel_local = jnp.repeat(jnp.where(picked, 0.0, BIG).astype(jnp.float32), BLK, axis=2)
    dqt, dk_local, dv_local, delta = local_attention(
        queries, keys, values, outputs, d_out, lse, sel_local)

    flat = table.reshape(devices * CAP)
    owner = jnp.arange(devices * CAP, dtype=jnp.int32) // CAP
    slot_seq = jnp.where(flat >= 0, flat // local_blocks, -1)
    slot_id = jnp.where(flat >= 0, owner * local_blocks + flat % local_blocks, -2)
    named = jnp.any(chosen[:, None] == slot_id[None, :, None, None], axis=3)
    named = named & (slot_seq[None, :, None] == jnp.arange(seqs, dtype=jnp.int32)[:, None, None])
    named = jnp.any(named, axis=0) & (owner != me)[:, None]
    slot_seq = jnp.where(jnp.any(named, axis=1), slot_seq, -1)
    sel_remote = jnp.repeat(jnp.where(named, 0.0, BIG).astype(jnp.float32), BLK, axis=1)
    sel_remote = jnp.concatenate([sel_remote, jnp.full((8, n), BIG, jnp.float32)], axis=0)[:, None, :]
    d_queries, gk, gv = remote_attention(slot_seq, queries, d_out, lse, delta, sel_remote, pk, pv, dqt)

    slots = devices * CAP
    back = jnp.concatenate(
        [gk[:slots].reshape(devices, CAP, BLK, ch), gv[:slots].reshape(devices, CAP, BLK, ch)], axis=1)
    back = lax.psum_scatter(back, "kv", scatter_dimension=0).astype(jnp.float32)
    hot = (served[:, None] == jnp.arange(own, dtype=jnp.int32)[None, :]).astype(jnp.float32)

    def finish(local, extra):
        full = local.reshape(own, BLK, ch).astype(jnp.float32)
        for c in range(CAP):
            full = full + hot[c][:, None, None] * extra[c][None]
        return full.astype(jnp.bfloat16).reshape(seqs, n, ch)

    d_keys = finish(dk_local, back[:CAP])
    d_values = finish(dv_local, back[CAP:])
    whole = lax.all_gather(layer_input, "tp", axis=2, tiled=True)
    d_weight = lax.dot_general(
        whole.reshape(seqs * n, whole.shape[2]), d_values.reshape(seqs * n, ch), TN,
        preferred_element_type=jnp.float32)
    d_weight = lax.psum_scatter(d_weight, "kv", scatter_dimension=0, tiled=True)
    return d_queries, d_keys, d_values, d_weight


def solution(mesh):
    spec = P(None, "kv", "tp")
    return jax.shard_map(
        body,
        mesh=mesh,
        in_specs=(spec,) * 7 + (P(None, "kv", None),),
        out_specs=(spec, spec, spec, P("kv", "tp")),
        check_vma=False,
    )
```

```python
import functools
import jax
import jax.numpy as jnp
from jax import lax
from jax.experimental import pallas as pl
from jax.experimental.pallas import tpu as pltpu
from jax.sharding import PartitionSpec as P

BLK = 64
CAP = 2
DH = 128
LOG2E = 1.4426950408889634
ROOT = DH ** -0.5
BIG = 1e30

NT = (((1,), (1,)), ((), ()))
TN = (((0,), (0,)), ((), ()))
NN = (((1,), (0,)), ((), ()))


def mm(a, b, dims):
    return lax.dot_general(a, b, dims, preferred_element_type=jnp.float32)


class Net:
    def __init__(self, send, recv):
        self.send, self.recv, self.n, self.all = send, recv, 0, []

    def copy(self, src, dst, kv):
        i = self.n
        self.n += 1
        c = pltpu.make_async_remote_copy(
            src_ref=src, dst_ref=dst, send_sem=self.send.at[i], recv_sem=self.recv.at[i],
            device_id=(kv, lax.axis_index("tp")), device_id_type=pl.DeviceIdType.MESH)
        c.start()
        self.all.append(c)
        return c

    def finish(self):
        for c in self.all:
            c.wait_send()


class Disk:
    def __init__(self, sems):
        self.sems, self.n, self.all = sems, 0, []

    def copy(self, src, dst):
        c = pltpu.make_async_copy(src, dst, self.sems.at[self.n])
        self.n += 1
        c.start()
        return c

    def keep(self, src, dst):
        self.all.append(self.copy(src, dst))

    def finish(self):
        for c in self.all:
            c.wait()


def place():
    me = lax.axis_index("kv")
    return me // 8, (me // 2) % 4, me % 2


def kv_of(z, y, c):
    return (z * 4 + y) * 2 + c


def barrier_with(peers):
    sem = pltpu.get_barrier_semaphore()
    for kv in peers:
        pl.semaphore_signal(sem, inc=1, device_id=(kv, lax.axis_index("tp")),
                            device_id_type=pl.DeviceIdType.MESH)
    pl.semaphore_wait(sem, len(peers))


class Gather:
    def __init__(self, net, disk, buf, out, cut, y_first):
        z, y, c = place()
        self.net, self.disk, self.buf, self.out, self.cut, self.y_first = net, disk, buf, out, cut, y_first
        f, s = (y, z) if y_first else (z, y)
        self.c = c
        self.f = [f, (f + 3) % 4, (f + 1) % 4, (f + 2) % 4]
        self.s = [s, (s + 3) % 4, (s + 1) % 4, (s + 2) % 4]
        self.side = []

    def at(self, f, s, c):
        return (c, s, f) if self.y_first else (c, f, s)

    def dev(self, f, s, c):
        return kv_of(s, f, c) if self.y_first else kv_of(f, s, c)

    def full(self, f, s, c=None):
        return self.buf.at[self.at(f, s, self.c if c is None else c)]

    def half(self, f, s, which):
        rows = pl.ds(0, self.cut) if which == 0 else pl.ds(self.cut, self.buf.shape[3] - self.cut)
        return self.buf.at[self.at(f, s, self.c) + (rows,)]

    def send(self, ref, f, s):
        return self.net.copy(ref, ref, self.dev(f, s, self.c))

    def have(self, f, s):
        ref = self.full(f, s)
        self.side.append((f, s, self.net.copy(ref, ref, self.dev(self.f[0], self.s[0], 1 - self.c))))
        self.disk.keep(ref, self.out.at[self.at(f, s, self.c)])

    def across(self, f):
        return (self.send(self.full(f, self.s[0]), self.f[0], self.s[2]),
                self.send(self.full(f, self.s[0]), self.f[0], self.s[1]))

    def phase0(self):
        own = self.full(self.f[0], self.s[0])
        self.a = self.send(own, self.f[2], self.s[0])
        self.b = self.send(own, self.f[1], self.s[0])
        self.second = [self.across(self.f[0])]
        self.have(self.f[0], self.s[0])

    def phase1(self):
        self.a.wait_recv()
        self.e = self.send(self.half(self.f[1], self.s[0], 0), self.f[2], self.s[0])
        self.second.append(self.across(self.f[1]))
        self.b.wait_recv()
        self.g = self.send(self.half(self.f[2], self.s[0], 1), self.f[1], self.s[0])
        self.second.append(self.across(self.f[2]))
        self.have(self.f[1], self.s[0])
        self.have(self.f[2], self.s[0])

    def phase2(self):
        self.e.wait_recv()
        self.g.wait_recv()
        self.second.append(self.across(self.f[3]))
        self.have(self.f[3], self.s[0])
        self.last = []

    def phase3(self, j):
        up, down = self.second[j]
        up.wait_recv()
        p = self.send(self.half(self.f[j], self.s[1], 0), self.f[0], self.s[2])
        down.wait_recv()
        q = self.send(self.half(self.f[j], self.s[2], 1), self.f[0], self.s[1])
        self.last.append((p, q))
        self.have(self.f[j], self.s[1])
        self.have(self.f[j], self.s[2])

    def phase4(self, j):
        for c in self.last[j]:
            c.wait_recv()
        self.have(self.f[j], self.s[3])

    def phase5(self):
        for f, s, c in self.side:
            c.wait_recv()
            self.disk.keep(self.full(f, s, 1 - self.c), self.out.at[self.at(f, s, 1 - self.c)])


def gather_kernel(need, lse_ref, sel_ref, q_hbm, k_hbm, v_hbm, o_hbm, do_hbm,
                  dqt_hbm, dk_hbm, dv_hbm, delta_ref, pk_hbm, pv_hbm, hot_ref,
                  qb, kb, vb, ob, dob, dqtb, dkb, dvb, pk, pv, rc, n1, ry, n2, rz,
                  send, recv, local):
    z, y, c = place()
    net, disk = Net(send, recv), Disk(local)
    loads = [disk.copy(a, b) for a, b in
             ((k_hbm, kb), (v_hbm, vb), (q_hbm, qb), (do_hbm, dob), (o_hbm, ob))]
    peers = [kv_of(z, y, 1 - c)]
    for d in range(1, 4):
        peers += [kv_of(z, (y + d) % 4, c), kv_of((z + d) % 4, y, c)]
    barrier_with(peers)
    first = net.copy(need.at[1 - c], rc, kv_of(z, y, 1 - c))
    for l in loads:
        l.wait()

    seqs, n, ch = qb.shape
    half = n // 2

    def unit(u, _):
        s = u // 2
        for g in range(2):
            h = (u % 2) * 2 + g
            hs = pl.ds(pl.multiple_of(h * DH, DH), DH)
            hr = pl.ds(h, 1)
            q = qb[s, :, hs]
            do = dob[s, :, hs]
            prod = do.astype(jnp.float32) * ob[s, :, hs].astype(jnp.float32)
            delta = jnp.sum(prod.T, axis=0, keepdims=True)
            delta_ref[s, hr, :] = delta
            lse = lse_ref[s, hr, :]
            parts = []
            for t in range(2):
                lo = t * half
                k = kb[s, pl.ds(lo, half), hs]
                v = vb[s, pl.ds(lo, half), hs]
                qc, doc = q[lo:], do[lo:]
                w = n - lo
                sc = mm(k, qc, NT)
                row = lax.broadcasted_iota(jnp.int32, (half, w), 0)
                col = lax.broadcasted_iota(jnp.int32, (half, w), 1)
                bias = jnp.concatenate(
                    [jnp.broadcast_to(lse[:, lo:] + sel_ref[s, j:j + 1, lo:], (BLK, w))
                     for j in range(lo // BLK, (lo + half) // BLK)], axis=0)
                p = jnp.exp2(jnp.where(row <= col, sc * (ROOT * LOG2E) - bias, -BIG))
                dp = mm(v, doc, NT)
                ds = (p * (dp - delta[:, lo:])).astype(jnp.bfloat16)
                dvb[s, pl.ds(lo, half), hs] = mm(p.astype(jnp.bfloat16), doc, NN).astype(jnp.bfloat16)
                dkb[s, pl.ds(lo, half), hs] = (mm(ds, qc, NN) * ROOT).astype(jnp.bfloat16)
                parts.append(mm(k, ds, TN))
            dqtb[s, hs, :half] = parts[0][:, :half]
            dqtb[s, hs, half:] = parts[0][:, half:] + parts[1]
        return 0

    def units(a, b):
        lax.fori_loop(a, b, unit, 0)

    units(0, 1)
    first.wait_recv()
    n1[...] = jnp.maximum(need[c], rc[...])
    ys = [net.copy(n1.at[(y + d) % 4], ry.at[d - 1], kv_of(z, (y + d) % 4, c)) for d in range(1, 4)]
    units(1, 2)
    for x in ys:
        x.wait_recv()
    n2[...] = jnp.maximum(jnp.maximum(n1[y], ry[0]), jnp.maximum(ry[1], ry[2]))
    zs = [net.copy(n2.at[(z + d) % 4], rz.at[d - 1], kv_of((z + d) % 4, y, c)) for d in range(1, 4)]
    units(2, 3)
    for x in zs:
        x.wait_recv()
    need1 = jnp.maximum(jnp.maximum(n2[z], rz[0]), jnp.maximum(rz[1], rz[2]))
    tri = (lax.broadcasted_iota(jnp.int32, (128, 128), 0) <=
           lax.broadcasted_iota(jnp.int32, (128, 128), 1))
    count = mm(need1.astype(jnp.bfloat16), tri.astype(jnp.float32).astype(jnp.bfloat16), NN)
    is0 = jnp.where((need1 > 0.5) & (count > 0.5) & (count < 1.5), 1.0, 0.0)
    is1 = jnp.where((need1 > 0.5) & (count > 1.5) & (count < 2.5), 1.0, 0.0)
    line = lax.broadcasted_iota(jnp.int32, (16, 128), 0)
    hot = jnp.where(line == 0, jnp.broadcast_to(is0[0:1], (16, 128)),
                    jnp.where(line == 1, jnp.broadcast_to(is1[0:1], (16, 128)), 0.0))
    hot = hot.astype(jnp.bfloat16)
    hot_ref[...] = hot
    pick_k = jnp.zeros((2 * BLK, ch), jnp.float32)
    pick_v = jnp.zeros((2 * BLK, ch), jnp.float32)
    for s in range(seqs):
        a = spread(hot, s, n)
        pick_k = pick_k + mm(a, kb[s], NN)
        pick_v = pick_v + mm(a, vb[s], NN)
    pk[c, z, y, :BLK] = pick_k[:BLK].astype(jnp.bfloat16)
    pk[c, z, y, BLK + 16:] = pick_k[BLK:].astype(jnp.bfloat16)
    pk[c, z, y, BLK:BLK + 16] = jnp.concatenate([hot] * (ch // 128), axis=1)
    pv[c, z, y] = pick_v.astype(jnp.bfloat16)

    gs = [Gather(net, disk, pk, pk_hbm, BLK + 16, True), Gather(net, disk, pv, pv_hbm, BLK, False)]
    for g in gs:
        g.phase0()
    units(3, 5)
    for g in gs:
        g.phase1()
    units(5, 6)
    for g in gs:
        g.phase2()
    for j in range(4):
        if j < 2:
            units(6 + j, 7 + j)
        for g in gs:
            g.phase3(j)
        if j == 1:
            disk.keep(dqtb, dqt_hbm)
            disk.keep(dkb, dk_hbm)
            disk.keep(dvb, dv_hbm)
    for j in range(4):
        for g in gs:
            g.phase4(j)
    for g in gs:
        g.phase5()
    net.finish()
    disk.finish()


def spread(hot, s, n):
    blocks = n // BLK
    b = lax.broadcasted_iota(jnp.int32, (128, n), 0)
    l = lax.broadcasted_iota(jnp.int32, (128, n), 1)
    rep = jnp.where(b == s * blocks + l // BLK, 1.0, 0.0).astype(jnp.bfloat16)
    wide = mm(hot, rep, NN)
    wide = jnp.where(b < BLK, jnp.broadcast_to(wide[0:1], (128, n)), jnp.broadcast_to(wide[1:2], (128, n)))
    return jnp.where(b % BLK == l % BLK, wide, 0.0).astype(jnp.bfloat16)


def gather_attention(need, lse, sel, q, k, v, o, do):
    seqs, n, ch = q.shape
    heads = ch // DH
    bf, f32 = jnp.bfloat16, jnp.float32
    whole = pl.BlockSpec(memory_space=pltpu.VMEM)
    hbm = pl.BlockSpec(memory_space=pl.ANY)
    return pl.pallas_call(
        gather_kernel,
        in_specs=[whole] * 3 + [hbm] * 5,
        out_specs=[hbm, hbm, hbm, whole, hbm, hbm, whole],
        out_shape=[
            jax.ShapeDtypeStruct((seqs, ch, n), f32),
            jax.ShapeDtypeStruct(q.shape, bf),
            jax.ShapeDtypeStruct(q.shape, bf),
            jax.ShapeDtypeStruct((seqs, heads, n), f32),
            jax.ShapeDtypeStruct((2, 4, 4, 2 * BLK + 16, ch), bf),
            jax.ShapeDtypeStruct((2, 4, 4, 2 * BLK, ch), bf),
            jax.ShapeDtypeStruct((16, 128), bf),
        ],
        scratch_shapes=[pltpu.VMEM(q.shape, bf)] * 5 + [
            pltpu.VMEM((seqs, ch, n), f32), pltpu.VMEM(q.shape, bf), pltpu.VMEM(q.shape, bf),
            pltpu.VMEM((2, 4, 4, 2 * BLK + 16, ch), bf), pltpu.VMEM((2, 4, 4, 2 * BLK, ch), bf),
            pltpu.VMEM((4, 4, 8, 128), f32), pltpu.VMEM((4, 4, 8, 128), f32),
            pltpu.VMEM((3, 4, 8, 128), f32), pltpu.VMEM((4, 8, 128), f32), pltpu.VMEM((3, 8, 128), f32),
            pltpu.SemaphoreType.DMA((80,)), pltpu.SemaphoreType.DMA((80,)), pltpu.SemaphoreType.DMA((80,)),
        ],
        compiler_params=pltpu.CompilerParams(
            vmem_limit_bytes=56 * 1024 * 1024, collective_id=0, has_side_effects=True),
        cost_estimate=pl.CostEstimate(flops=20_000_000_000, bytes_accessed=30 << 20, transcendentals=1 << 22),
        name="gather_attention",
    )(need, lse, sel, q, k, v, o, do)


class Route:
    def __init__(self, net, buf, rows, y_first, slots):
        z, y, c = place()
        self.net, self.buf, self.rows, self.y_first = net, buf, rows, y_first
        self.ra, self.rb, self.rp, self.rm, self.e, self.ta, self.tb, self.tp, self.tm = slots
        f, s = (y, z) if y_first else (z, y)
        self.c, self.f, self.s = c, f, s
        self.wide = buf.shape[-1] // 2

    def dev(self, f, s):
        return kv_of(s, f, self.c) if self.y_first else kv_of(f, s, self.c)

    def src(self, f, part=None):
        lanes = pl.ds(0, 2 * self.wide) if part is None else pl.ds(part * self.wide, self.wide)
        if self.y_first:
            return self.buf.at[:, f, self.rows, lanes]
        return self.buf.at[f, :, self.rows, lanes]

    def step1(self):
        f, s = self.f, self.s
        self.c1 = (self.net.copy(self.src((f + 2) % 4, 0), self.ra, self.dev((f + 1) % 4, s)),
                   self.net.copy(self.src((f + 2) % 4, 1), self.rb, self.dev((f + 3) % 4, s)))

    def step2(self):
        f, s, w = self.f, self.s, self.wide
        self.c2 = []
        for i, (d, got, dst) in enumerate(((1, self.ra, self.rp), (3, self.rb, self.rm))):
            self.c1[i].wait_recv()
            at = self.src((f + d) % 4, i)
            at[...] = (at[...].astype(jnp.float32) + got[...].astype(jnp.float32)).astype(jnp.bfloat16)
            self.c2.append(self.net.copy(self.src((f + d) % 4), dst, self.dev((f + d) % 4, s)))

    def step3(self):
        f, s, w = self.f, self.s, self.wide
        for x in self.c2:
            x.wait_recv()
        total = self.src(f)[...].astype(jnp.float32) + self.rp[...].astype(jnp.float32)
        self.e[...] = (total + self.rm[...].astype(jnp.float32)).astype(jnp.bfloat16)
        far = (s + 2) % 4
        self.c3 = (self.net.copy(self.e.at[far, :, pl.ds(0, w)], self.ta, self.dev(f, (s + 1) % 4)),
                   self.net.copy(self.e.at[far, :, pl.ds(w, w)], self.tb, self.dev(f, (s + 3) % 4)))

    def step4(self):
        f, s, w = self.f, self.s, self.wide
        self.c4 = []
        for i, (d, got, dst) in enumerate(((1, self.ta, self.tp), (3, self.tb, self.tm))):
            self.c3[i].wait_recv()
            at = self.e.at[(s + d) % 4, :, pl.ds(i * w, w)]
            at[...] = (at[...].astype(jnp.float32) + got[...].astype(jnp.float32)).astype(jnp.bfloat16)
            self.c4.append(self.net.copy(self.e.at[(s + d) % 4], dst, self.dev(f, (s + d) % 4)))

    def step5(self):
        for x in self.c4:
            x.wait_recv()
        total = self.e[self.s].astype(jnp.float32) + self.tp[...].astype(jnp.float32)
        return total + self.tm[...].astype(jnp.float32)


def route_scratch(rows, ch):
    bf = jnp.bfloat16
    return [pltpu.VMEM((4, rows, ch // 2), bf), pltpu.VMEM((4, rows, ch // 2), bf),
            pltpu.VMEM((4, rows, ch), bf), pltpu.VMEM((4, rows, ch), bf), pltpu.VMEM((4, rows, ch), bf),
            pltpu.VMEM((rows, ch // 2), bf), pltpu.VMEM((rows, ch // 2), bf),
            pltpu.VMEM((rows, ch), bf), pltpu.VMEM((rows, ch), bf)]


class Stream:
    def __init__(self, net, buf, slots):
        rows = buf.shape[2] // 2
        self.rows = rows
        self.routes = [Route(net, buf, pl.ds(0, rows), True, slots[:9]),
                       Route(net, buf, pl.ds(rows, rows), False, slots[9:])]

    def run(self, name):
        return [getattr(r, name)() for r in self.routes]


def reduce_kernel(hot_ref, gk_hbm, gv_hbm, dv_hbm, x_hbm, fk_ref, fv_ref, dw_ref,
                  mk, mv, rk, rv, dvb, xb, wf, ws, wr, wb, *rest):
    ks, vs, wslots = rest[0:18], rest[18:36], rest[36:54]
    send, recv, local = rest[54:]
    z, y, c = place()
    net, disk = Net(send, recv), Disk(local)
    mine, other = pl.ds(c * 16, 16), pl.ds((1 - c) * 16, 16)
    load_v = disk.copy(gv_hbm.at[mine], mv)
    load_k = disk.copy(gk_hbm.at[mine], mk)
    load_d = disk.copy(dv_hbm, dvb)
    load_x = [disk.copy(x_hbm.at[t], xb.at[t]) for t in range(4)]
    peers = [kv_of(z, y, 1 - c)]
    for d in (1, 3):
        peers += [kv_of(z, (y + d) % 4, c), kv_of((z + d) % 4, y, c)]
    barrier_with(peers)
    partner = kv_of(z, y, 1 - c)
    side_v = net.copy(gv_hbm.at[other], rv, partner)
    side_k = net.copy(gk_hbm.at[other], rk, partner)

    def fold(dst, src, parts):
        def step(i, _):
            dst[i] = (dst[i].astype(jnp.float32) + src[i].astype(jnp.float32)).astype(jnp.bfloat16)
            return 0
        lax.fori_loop(0, parts, step, 0)

    bv = mv.reshape(4, 4, mv.shape[1], mv.shape[2])
    bk = mk.reshape(4, 4, mk.shape[1], mk.shape[2])
    v, k = Stream(net, bv, vs), Stream(net, bk, ks)
    seqs, n, ch = dvb.shape

    def product(t):
        load_x[t].wait()

        def step(s, _):
            wf[t] = wf[t] + mm(xb[t, s], dvb[s], TN)
            return 0

        wf[t] = mm(xb[t, 0], dvb[0], TN)
        lax.fori_loop(1, seqs, step, 0)

    load_v.wait()
    side_v.wait_recv()
    fold(mv, rv, 16)
    v.run("step1")
    load_k.wait()
    side_k.wait_recv()
    fold(mk, rk, 16)
    k.run("step1")
    load_d.wait()
    hot = hot_ref[...]
    v.run("step2")
    product(0)
    k.run("step2")
    product(1)
    v.run("step3")
    product(2)
    v.run("step4")
    product(3)
    old = jnp.zeros((2 * BLK, ch), jnp.float32)
    xs = [jnp.zeros((2 * BLK, ch), jnp.float32) for t in range(4)]
    for s in range(seqs):
        a = spread(hot, s, n)
        old = old + mm(a, dvb[s], NN)
        xs = [x + mm(a, xb[t, s], NN) for t, x in enumerate(xs)]
    top, low = v.run("step5")
    fv_ref[:BLK] = top
    fv_ref[BLK:] = low
    extra = jnp.concatenate([top, low], axis=0)
    diff = ((old + extra).astype(jnp.bfloat16).astype(jnp.float32) - old).astype(jnp.bfloat16)
    for t in range(4):
        wf[t] = wf[t] + mm(xs[t].astype(jnp.bfloat16), diff, TN)
        for j in range(4):
            ws[t * 4 + j] = wf[t, pl.ds(pl.multiple_of(j * 128 + (1 - c) * BLK, BLK), BLK)].astype(jnp.bfloat16)
    side_w = net.copy(ws, wr, partner)
    k.run("step3")
    side_w.wait_recv()
    for t in range(4):
        for j in range(4):
            own = wf[t, pl.ds(pl.multiple_of(j * 128 + c * BLK, BLK), BLK)]
            wb[t, j] = (own + wr[t * 4 + j].astype(jnp.float32)).astype(jnp.bfloat16)
    w = Stream(net, wb, wslots)
    w.run("step1")
    k.run("step4")
    w.run("step2")
    top, low = k.run("step5")
    fk_ref[:BLK] = top
    fk_ref[BLK:] = low
    w.run("step3")
    w.run("step4")
    top, low = w.run("step5")
    dw_ref[:BLK // 2] = top
    dw_ref[BLK // 2:] = low
    net.finish()


def reduce_weight(hot, gk, gv, dv, x):
    seqs, n, ch = dv.shape
    bf, f32 = jnp.bfloat16, jnp.float32
    whole = pl.BlockSpec(memory_space=pltpu.VMEM)
    hbm = pl.BlockSpec(memory_space=pl.ANY)
    part = pltpu.VMEM((16, 2 * BLK, ch), bf)
    return pl.pallas_call(
        reduce_kernel,
        in_specs=[whole] + [hbm] * 4,
        out_specs=[whole] * 3,
        out_shape=[
            jax.ShapeDtypeStruct((2 * BLK, ch), f32),
            jax.ShapeDtypeStruct((2 * BLK, ch), f32),
            jax.ShapeDtypeStruct((BLK, ch), f32),
        ],
        scratch_shapes=[part] * 4 + [
            pltpu.VMEM(dv.shape, bf), pltpu.VMEM(x.shape, bf), pltpu.VMEM((4, n, ch), f32),
            pltpu.VMEM((16, BLK, ch), bf), pltpu.VMEM((16, BLK, ch), bf), pltpu.VMEM((4, 4, BLK, ch), bf),
        ] + route_scratch(BLK, ch) * 4 + route_scratch(BLK // 2, ch) * 2 + [
            pltpu.SemaphoreType.DMA((60,)), pltpu.SemaphoreType.DMA((60,)), pltpu.SemaphoreType.DMA((8,)),
        ],
        compiler_params=pltpu.CompilerParams(
            vmem_limit_bytes=56 * 1024 * 1024, collective_id=1, has_side_effects=True),
        cost_estimate=pl.CostEstimate(flops=20_000_000_000, bytes_accessed=20 << 20, transcendentals=0),
        name="reduce_weight",
    )(hot, gk, gv, dv, x)


def remote_kernel(seq_ref, q_ref, do_ref, lse_ref, delta_ref, sel_ref, pk_ref, pv_ref, dqt_in,
                  dq_ref, gk_ref, gv_ref, acc, list_ref, cnt_ref):
    seqs = 4
    heads = q_ref.shape[2] // DH
    slots = 2 * pk_ref.shape[0]
    s = pl.program_id(0)

    @pl.when(s == 0)
    def _():
        for t in range(seqs):
            cnt_ref[t] = 0

        def scan(i, _):
            t = seq_ref[i]

            @pl.when(t >= 0)
            def _():
                c = cnt_ref[t]
                list_ref[t, c] = i
                cnt_ref[t] = c + 1

            @pl.when(t < 0)
            def _():
                gk_ref[i] = jnp.zeros(gk_ref.shape[1:], gk_ref.dtype)
                gv_ref[i] = jnp.zeros(gv_ref.shape[1:], gv_ref.dtype)
            return 0

        lax.fori_loop(0, slots, scan, 0)

    acc[...] = dqt_in[0]
    n = cnt_ref[s]

    def chunk(c, _):
        ids = []
        for e in range(4):
            at = c * 4 + e
            i = list_ref[s, jnp.minimum(at, n - 1)]
            ids.append((i, jnp.where(at < n, i, slots)))
        for h in range(heads):
            hs = slice(h * DH, (h + 1) * DH)
            q = q_ref[0, :, hs]
            do = do_ref[0, :, hs]
            k = jnp.concatenate([pk_ref[i // 2, pl.ds(pl.multiple_of(i % 2 * 80, 16), BLK), hs] for i, _ in ids], axis=0)
            v = jnp.concatenate([pv_ref[i // 2, pl.ds(pl.multiple_of(i % 2 * BLK, BLK), BLK), hs] for i, _ in ids], axis=0)
            lse = lse_ref[0, h:h + 1, :]
            st = mm(k, q, NT)
            bias = jnp.concatenate(
                [jnp.broadcast_to(lse + sel_ref[j], (BLK, lse.shape[1])) for _, j in ids], axis=0)
            p = jnp.exp2(st * (ROOT * LOG2E) - bias)
            dp = mm(v, do, NT)
            ds = (p * (dp - delta_ref[0, h:h + 1, :])).astype(jnp.bfloat16)
            dv = mm(p.astype(jnp.bfloat16), do, NN).astype(jnp.bfloat16)
            dk = (mm(ds, q, NN) * ROOT).astype(jnp.bfloat16)
            for e, (_, j) in enumerate(ids):
                gv_ref[j, :, hs] = dv[e * BLK:(e + 1) * BLK]
                gk_ref[j, :, hs] = dk[e * BLK:(e + 1) * BLK]
            acc[hs, :] += mm(k, ds, TN)
        return 0

    lax.fori_loop(0, (n + 3) // 4, chunk, 0)
    for h in range(heads):
        hs = slice(h * DH, (h + 1) * DH)
        dq_ref[0, :, hs] = (acc[hs, :].T * ROOT).astype(jnp.bfloat16)


def remote_attention(slot_seq, q, do, lse, delta, sel, pk, pv, dqt):
    seqs, n, ch = q.shape
    heads = ch // DH
    slots = 2 * pk.shape[0]
    big = pl.BlockSpec((1, n, ch), lambda s: (s, 0, 0))
    small = pl.BlockSpec((1, heads, n), lambda s: (s, 0, 0))
    whole = pl.BlockSpec(memory_space=pltpu.VMEM)
    return pl.pallas_call(
        remote_kernel,
        grid=(seqs,),
        in_specs=[pl.BlockSpec(memory_space=pltpu.SMEM), big, big, small, small, whole, whole, whole,
                  pl.BlockSpec((1, ch, n), lambda s: (s, 0, 0))],
        out_specs=[big, whole, whole],
        out_shape=[
            jax.ShapeDtypeStruct(q.shape, jnp.bfloat16),
            jax.ShapeDtypeStruct((slots + 2, BLK, ch), jnp.bfloat16),
            jax.ShapeDtypeStruct((slots + 2, BLK, ch), jnp.bfloat16),
        ],
        scratch_shapes=[
            pltpu.VMEM((ch, n), jnp.float32),
            pltpu.SMEM((seqs, slots), jnp.int32),
            pltpu.SMEM((seqs,), jnp.int32),
        ],
        compiler_params=pltpu.CompilerParams(vmem_limit_bytes=60 * 1024 * 1024),
        cost_estimate=pl.CostEstimate(flops=5 * 2 * heads * slots * BLK * n * DH, bytes_accessed=28 << 20,
                                      transcendentals=heads * slots * BLK * n),
        name="remote_attention",
    )(slot_seq, q, do, lse, delta, sel, pk, pv, dqt)


def body(layer_input, queries, keys, values, outputs, d_out, log_sums, chosen):
    seqs, n, ch = queries.shape
    local_blocks = n // BLK
    devices = lax.axis_size("kv")
    me = lax.axis_index("kv")
    own = seqs * local_blocks
    lse = jnp.swapaxes(log_sums, 1, 2) * LOG2E
    whole = lax.all_gather(layer_input, "tp", axis=0)

    in_use = chosen >= 0
    remote = in_use & (chosen // local_blocks != me)
    ids = jnp.arange(devices * local_blocks, dtype=jnp.int32)
    needed = jnp.max(((chosen[..., None] == ids) & remote[..., None]).astype(jnp.float32), axis=(1, 2))
    needed = needed.reshape(seqs, 4, 4, 2, local_blocks).transpose(3, 2, 1, 0, 4).reshape(2, 4, 4, 1, own)
    needed = jnp.pad(jnp.broadcast_to(needed, (2, 4, 4, 8, own)), ((0, 0),) * 4 + ((0, 128 - own),))
    mine = me * local_blocks + jnp.arange(local_blocks, dtype=jnp.int32)
    picked = jnp.any(chosen[:, None, :, :] == mine[None, :, None, None], axis=3)
    sel_local = jnp.repeat(jnp.where(picked, 0.0, BIG).astype(jnp.float32), BLK, axis=2)
    dqt, dk_local, dv_local, delta, pk, pv, hot = gather_attention(
        needed, lse, sel_local, queries, keys, values, outputs, d_out)

    pk = pk.reshape(devices, 2 * BLK + 16, ch)
    pv = pv.reshape(devices, 2 * BLK, ch)
    table = pk[:, BLK:BLK + CAP, :own].astype(jnp.float32)
    place_of = jnp.sum(table * jnp.arange(own, dtype=jnp.float32), axis=2).astype(jnp.int32)
    flat = jnp.where(jnp.sum(table, axis=2) > 0.5, place_of, -1).reshape(devices * CAP)
    order = jnp.arange(devices * CAP, dtype=jnp.int32) // CAP
    owner = (order % (devices // 2)) * 2 + order // (devices // 2)
    slot_seq = jnp.where(flat >= 0, flat // local_blocks, -1)
    slot_id = jnp.where(flat >= 0, owner * local_blocks + flat % local_blocks, -2)
    named = jnp.any(chosen[:, None] == slot_id[None, :, None, None], axis=3)
    named = named & (slot_seq[None, :, None] == jnp.arange(seqs, dtype=jnp.int32)[:, None, None])
    named = jnp.any(named, axis=0) & (owner != me)[:, None]
    slot_seq = jnp.where(jnp.any(named, axis=1), slot_seq, -1)
    sel_remote = jnp.repeat(jnp.where(named, 0.0, BIG).astype(jnp.float32), BLK, axis=1)
    sel_remote = jnp.concatenate([sel_remote, jnp.full((8, n), BIG, jnp.float32)], axis=0)[:, None, :]
    d_queries, gk, gv = remote_attention(slot_seq, queries, d_out, lse, delta, sel_remote, pk, pv, dqt)

    gk = gk.reshape(devices + 1, CAP * BLK, ch)
    gv = gv.reshape(devices + 1, CAP * BLK, ch)
    back_k, back_v, d_weight = reduce_weight(hot, gk, gv, dv_local, whole)
    serve = hot[:CAP, :own].astype(jnp.float32)

    def finish(local, extra):
        full = local.reshape(own, BLK, ch).astype(jnp.float32)
        for c in range(CAP):
            full = full + serve[c][:, None, None] * extra[c * BLK:(c + 1) * BLK][None]
        return full.astype(jnp.bfloat16).reshape(seqs, n, ch)

    return d_queries, finish(dk_local, back_k), finish(dv_local, back_v), d_weight


def solution(mesh):
    spec = P(None, "kv", "tp")
    return jax.shard_map(
        body,
        mesh=mesh,
        in_specs=(spec,) * 7 + (P(None, "kv", None),),
        out_specs=(spec, spec, spec, P("kv", "tp")),
        check_vma=False,
    )
```

```python
import functools
import jax
import jax.numpy as jnp
from jax import lax
from jax.experimental import pallas as pl
from jax.experimental.pallas import tpu as pltpu
from jax.sharding import PartitionSpec as P

BLK = 64
CAP = 2
DH = 128
LOG2E = 1.4426950408889634
ROOT = DH ** -0.5
BIG = 1e30

NT = (((1,), (1,)), ((), ()))
TN = (((0,), (0,)), ((), ()))
NN = (((1,), (0,)), ((), ()))


def mm(a, b, dims):
    return lax.dot_general(a, b, dims, preferred_element_type=jnp.float32)


class Net:
    def __init__(self, send, recv):
        self.send, self.recv, self.n, self.all = send, recv, 0, []

    def copy(self, src, dst, kv, tp=None):
        i = self.n
        self.n += 1
        c = pltpu.make_async_remote_copy(
            src_ref=src, dst_ref=dst, send_sem=self.send.at[i], recv_sem=self.recv.at[i],
            device_id=(kv, lax.axis_index("tp") if tp is None else tp), device_id_type=pl.DeviceIdType.MESH)
        c.start()
        self.all.append(c)
        return c

    def finish(self):
        for c in self.all:
            c.wait_send()


class Disk:
    def __init__(self, sems):
        self.sems, self.n, self.all = sems, 0, []

    def copy(self, src, dst):
        c = pltpu.make_async_copy(src, dst, self.sems.at[self.n])
        self.n += 1
        c.start()
        return c

    def keep(self, src, dst):
        self.all.append(self.copy(src, dst))

    def finish(self):
        for c in self.all:
            c.wait()


def place():
    me = lax.axis_index("kv")
    return me // 8, (me // 2) % 4, me % 2


def kv_of(z, y, c):
    return (z * 4 + y) * 2 + c


def barrier_with(peers, across):
    sem = pltpu.get_barrier_semaphore()
    for kv in peers:
        pl.semaphore_signal(sem, inc=1, device_id=(kv, lax.axis_index("tp")),
                            device_id_type=pl.DeviceIdType.MESH)
    for tp in across:
        pl.semaphore_signal(sem, inc=1, device_id=(lax.axis_index("kv"), tp),
                            device_id_type=pl.DeviceIdType.MESH)
    pl.semaphore_wait(sem, len(peers) + len(across))


class Gather:
    def __init__(self, net, buf, y_first):
        z, y, c = place()
        self.net, self.buf, self.y_first = net, buf, y_first
        f, s = (y, z) if y_first else (z, y)
        self.c = c
        self.f = [f, (f + 3) % 4, (f + 1) % 4, (f + 2) % 4]
        self.s = [s, (s + 3) % 4, (s + 1) % 4, (s + 2) % 4]
        self.side, self.sent = [], []

    def full(self, f, s, c=None):
        c = self.c if c is None else c
        return self.buf.at[(c, s, f) if self.y_first else (c, f, s)]

    def half(self, f, s, which):
        c = self.c
        return self.buf.at[(c, s, f, which) if self.y_first else (c, f, s, which)]

    def send(self, ref, f, s, c=None):
        c = self.c if c is None else c
        x = self.net.copy(ref, ref, kv_of(s, f, c) if self.y_first else kv_of(f, s, c))
        self.sent.append(x)
        return x

    def have(self, f, s):
        self.side.append(self.send(self.full(f, s), self.f[0], self.s[0], 1 - self.c))

    def across(self, f):
        return (self.send(self.full(f, self.s[0]), self.f[0], self.s[2]),
                self.send(self.full(f, self.s[0]), self.f[0], self.s[1]))

    def phase0(self):
        own = self.full(self.f[0], self.s[0])
        self.a = self.send(own, self.f[2], self.s[0])
        self.b = self.send(own, self.f[1], self.s[0])
        self.second = [self.across(self.f[0])]
        self.have(self.f[0], self.s[0])

    def phase1(self):
        self.a.wait_recv()
        self.e = self.send(self.half(self.f[1], self.s[0], 0), self.f[2], self.s[0])
        self.second.append(self.across(self.f[1]))
        self.b.wait_recv()
        self.g = self.send(self.half(self.f[2], self.s[0], 1), self.f[1], self.s[0])
        self.second.append(self.across(self.f[2]))
        self.have(self.f[1], self.s[0])
        self.have(self.f[2], self.s[0])

    def phase2(self):
        self.e.wait_recv()
        self.g.wait_recv()
        self.second.append(self.across(self.f[3]))
        self.have(self.f[3], self.s[0])
        self.last = []

    def phase3(self, j):
        up, down = self.second[j]
        up.wait_recv()
        p = self.send(self.half(self.f[j], self.s[1], 0), self.f[0], self.s[2])
        down.wait_recv()
        q = self.send(self.half(self.f[j], self.s[2], 1), self.f[0], self.s[1])
        self.last.append((p, q))
        self.have(self.f[j], self.s[1])
        self.have(self.f[j], self.s[2])

    def phase4(self, j):
        for c in self.last[j]:
            c.wait_recv()
        self.have(self.f[j], self.s[3])

    def phase5(self):
        for c in self.side:
            c.wait_recv()

    def drain(self):
        for c in self.sent:
            c.wait_send()


class Route:
    def __init__(self, net, buf, rows, y_first, slots):
        z, y, c = place()
        self.net, self.buf, self.rows, self.y_first = net, buf, rows, y_first
        self.ra, self.rb, self.rp, self.rm, self.e, self.ta, self.tb, self.tp, self.tm = slots
        self.c = c
        self.f, self.s = (y, z) if y_first else (z, y)
        self.wide = buf.shape[-1] // 2
        self.kind = self.e.dtype

    def dev(self, f, s):
        return kv_of(s, f, self.c) if self.y_first else kv_of(f, s, self.c)

    def src(self, f, part=None):
        lanes = pl.ds(0, 2 * self.wide) if part is None else pl.ds(part * self.wide, self.wide)
        if self.y_first:
            return self.buf.at[:, f, self.rows, :, lanes]
        return self.buf.at[f, :, self.rows, :, lanes]

    def step1(self):
        f, s = self.f, self.s
        self.c1 = (self.net.copy(self.src((f + 2) % 4, 0), self.ra, self.dev((f + 1) % 4, s)),
                   self.net.copy(self.src((f + 2) % 4, 1), self.rb, self.dev((f + 3) % 4, s)))

    def step2(self):
        f, s, w = self.f, self.s, self.wide
        self.c2 = []
        for i, (d, got, dst) in enumerate(((1, self.ra, self.rp), (3, self.rb, self.rm))):
            self.c1[i].wait_recv()
            at = self.src((f + d) % 4, i)
            at[...] = (at[...].astype(jnp.float32) + got[...].astype(jnp.float32)).astype(jnp.bfloat16)
            self.c2.append(self.net.copy(self.src((f + d) % 4), dst, self.dev((f + d) % 4, s)))

    def step3(self):
        f, s, w = self.f, self.s, self.wide
        for x in self.c2:
            x.wait_recv()
        total = self.src(f)[...].astype(jnp.float32) + self.rp[...].astype(jnp.float32)
        self.e[...] = (total + self.rm[...].astype(jnp.float32)).astype(self.kind)
        far = (s + 2) % 4
        self.c3 = (self.net.copy(self.e.at[far, :, pl.ds(0, w)], self.ta, self.dev(f, (s + 1) % 4)),
                   self.net.copy(self.e.at[far, :, pl.ds(w, w)], self.tb, self.dev(f, (s + 3) % 4)))

    def step4(self):
        f, s, w = self.f, self.s, self.wide
        self.c4 = []
        for i, (d, got, dst) in enumerate(((1, self.ta, self.tp), (3, self.tb, self.tm))):
            self.c3[i].wait_recv()
            at = self.e.at[(s + d) % 4, :, pl.ds(i * w, w)]
            at[...] = (at[...].astype(jnp.float32) + got[...].astype(jnp.float32)).astype(self.kind)
            self.c4.append(self.net.copy(self.e.at[(s + d) % 4], dst, self.dev(f, (s + d) % 4)))

    def step5(self):
        for x in self.c4:
            x.wait_recv()
        total = self.e[self.s].astype(jnp.float32) + self.tp[...].astype(jnp.float32)
        return total + self.tm[...].astype(jnp.float32)


def route_scratch(rows, ch, kind):
    bf = jnp.bfloat16
    return [pltpu.VMEM((4, rows, ch // 2), bf), pltpu.VMEM((4, rows, ch // 2), bf),
            pltpu.VMEM((4, rows, ch), bf), pltpu.VMEM((4, rows, ch), bf), pltpu.VMEM((4, rows, ch), kind),
            pltpu.VMEM((rows, ch // 2), kind), pltpu.VMEM((rows, ch // 2), kind),
            pltpu.VMEM((rows, ch), kind), pltpu.VMEM((rows, ch), kind)]


class Stream:
    def __init__(self, net, buf, slots):
        self.routes = [Route(net, buf, 0, True, slots[:9]), Route(net, buf, 1, False, slots[9:])]

    def run(self, name):
        return [getattr(r, name)() for r in self.routes]


class Ring:
    def __init__(self, net, own, everyone):
        self.net, self.own, self.all = net, own, everyone
        t = lax.axis_index("tp")
        self.t = [t, (t + 3) % 4, (t + 1) % 4, (t + 2) % 4]
        self.onward = []

    def start(self):
        t = self.t
        self.up, self.down = [], []
        for j in range(4):
            self.up.append(self.copy(self.own.at[j], self.all.at[t[0], j], t[2]))
            i = (j + 2) % 4
            self.down.append(self.copy(self.own.at[i], self.all.at[t[0], i], t[1]))

    def copy(self, src, dst, tp):
        return self.net.copy(src, dst, lax.axis_index("kv"), tp)

    def pass_on(self, j):
        self.up[j].wait_recv()
        at = self.all.at[self.t[1], j]
        self.onward.append(self.copy(at, at, self.t[2]))
        self.down[j].wait_recv()
        at = self.all.at[self.t[2], j + 2]
        self.onward.append(self.copy(at, at, self.t[1]))

    def near(self):
        for c in self.up[2:] + self.down[2:]:
            c.wait_recv()

    def far(self):
        for c in self.onward:
            c.wait_recv()


def whole_kernel(code_ref, lse_ref, pick_ref, q_hbm, k_hbm, v_hbm, o_hbm, do_hbm, x_hbm,
                 dq_hbm, dk_hbm, dv_hbm, dw_ref, xall_hbm,
                 qb, kb, vb, ob, dob, dqt, dkb, dvb, dqb, delta_ref,
                 need, rc, n1, ry, n2, rz, tab, pka, pva, pkb, pvb, gk, gv, part,
                 info, spots, info_s, spots_s, to_s, rka, rva, rkb, rvb, ws, wr, wb, *rest):
    kas, vas, kbs, vbs, wslots = (rest[i * 18:i * 18 + 18] for i in range(5))
    send, recv, local = rest[90:]
    z, y, c = place()
    me = lax.axis_index("kv")
    net, disk = Net(send, recv), Disk(local)
    loads = [disk.copy(a, b) for a, b in
             ((k_hbm, kb), (v_hbm, vb), (q_hbm, qb), (do_hbm, dob), (o_hbm, ob))]
    partner = kv_of(z, y, 1 - c)
    peers = [partner]
    for d in range(1, 4):
        peers += [kv_of(z, (y + d) % 4, c), kv_of((z + d) % 4, y, c)]
    x = Ring(net, x_hbm, xall_hbm)
    barrier_with(peers, x.t[1:3])

    seqs, n, ch = qb.shape
    half = n // 2

    def six(ref):
        return ref.reshape(2, 4, 4, CAP, BLK, ch // 2)

    blocks = n // BLK
    wide = ch // 2
    slots = 32 * CAP
    room = 18

    flat = (lax.broadcasted_iota(jnp.int32, (32, 128), 0) * 128 +
            lax.broadcasted_iota(jnp.int32, (32, 128), 1))

    def mark(i, seen):
        for j in range(8):
            seen = jnp.where(flat == code_ref[i * 8 + j], 1, seen)
        return seen

    seen = lax.fori_loop(0, code_ref.shape[0] // 8, mark, jnp.zeros((32, 128), jnp.int32))
    for i in range(32):
        need[i // 16, i // 4 % 4, i % 4] = jnp.broadcast_to(seen[i:i + 1], (8, 128))
    first = net.copy(need.at[1 - c], rc, partner)
    x.start()
    for l in loads:
        l.wait()

    def bias_row(lse, s, block):
        hit = jnp.max(jnp.where(pick_ref[s] == block, 1, 0), axis=0, keepdims=True)
        return jnp.where(hit > 0, lse, BIG)

    def unit(u, _):
        s = u // 2
        for g in range(2):
            h = (u % 2) * 2 + g
            hs = pl.ds(pl.multiple_of(h * DH, DH), DH)
            hr = pl.ds(h, 1)
            q = qb[s, :, hs]
            do = dob[s, :, hs]
            prod = do.astype(jnp.float32) * ob[s, :, :, hs].reshape(n, DH).astype(jnp.float32)
            delta = jnp.sum(prod.T, axis=0, keepdims=True)
            delta_ref[s, hr, :] = delta
            lse = lse_ref[s, hr, :]
            parts = []
            for t in range(2):
                lo = t * half
                here = slice(lo // BLK, (lo + half) // BLK)
                k = kb[s, here, :, hs].reshape(half, DH)
                v = vb[s, here, :, hs].reshape(half, DH)
                qc, doc = q[lo:], do[lo:]
                w = n - lo
                sc = mm(k, qc, NT)
                row = lax.broadcasted_iota(jnp.int32, (half, w), 0)
                col = lax.broadcasted_iota(jnp.int32, (half, w), 1)
                bias = jnp.concatenate(
                    [jnp.broadcast_to(bias_row(lse, s, me * blocks + j)[:, lo:], (BLK, w))
                     for j in range(lo // BLK, (lo + half) // BLK)], axis=0)
                p = jnp.exp2(jnp.where(row <= col, sc * (ROOT * LOG2E) - bias, -BIG))
                dp = mm(v, doc, NT)
                ds = (p * (dp - delta[:, lo:])).astype(jnp.bfloat16)
                dvb[s, here, :, hs] = mm(p.astype(jnp.bfloat16), doc, NN).astype(jnp.bfloat16).reshape(-1, BLK, DH)
                dkb[s, here, :, hs] = (mm(ds, qc, NN) * ROOT).astype(jnp.bfloat16).reshape(-1, BLK, DH)
                parts.append(mm(k, ds, TN))
            dqt[s, hs, :half] = parts[0][:, :half]
            dqt[s, hs, half:] = parts[0][:, half:] + parts[1]
        return 0

    def units(a, b):
        lax.fori_loop(a, b, unit, 0)

    units(0, 1)
    first.wait_recv()
    n1[...] = jnp.maximum(need[c], rc[...])
    ys = [net.copy(n1.at[(y + d) % 4], ry.at[d - 1], kv_of(z, (y + d) % 4, c)) for d in range(1, 4)]
    units(1, 2)
    for a in ys:
        a.wait_recv()
    n2[...] = jnp.maximum(jnp.maximum(n1[y], ry[0]), jnp.maximum(ry[1], ry[2]))
    zs = [net.copy(n2.at[(z + d) % 4], rz.at[d - 1], kv_of((z + d) % 4, y, c)) for d in range(1, 4)]
    units(2, 3)
    for a in zs:
        a.wait_recv()
    need1 = jnp.maximum(jnp.maximum(n2[z], rz[0]), jnp.maximum(rz[1], rz[2]))
    info[...] = need1
    disk.copy(info, info_s).wait()

    def first_two(i, state):
        seen, s0, s1 = state
        here = info_s[0, i]
        s0 = jnp.where((here == 1) & (seen == 0), i, s0)
        s1 = jnp.where((here == 1) & (seen == 1), i, s1)
        return seen + here, s0, s1

    minus = jnp.int32(-1)
    _, served0, served1 = lax.fori_loop(0, seqs * blocks, first_two, (jnp.int32(0), minus, minus))
    served = (served0, served1)
    lane8 = lax.broadcasted_iota(jnp.int32, (8, 128), 1)
    tab[c, z, y] = jnp.where(lane8 == 0, served0, jnp.where(lane8 == 1, served1, minus))
    tys = [net.copy(tab.at[c, z, y], tab.at[c, z, y], kv_of(z, (y + d) % 4, c)) for d in range(1, 4)]

    def rows_of(ref):
        out = []
        for b in served:
            b = jnp.clip(b, 0, seqs * blocks - 1)
            out.append(ref[b // blocks, b % blocks])
        return out

    for b, (pick_k, pick_v) in enumerate(zip(rows_of(kb), rows_of(vb))):
        at = (c * 16 + z * 4 + y) * CAP + b
        pka[at] = pick_k[:, :wide]
        pva[at] = pick_v[:, :wide]
        pkb[at] = pick_k[:, wide:]
        pvb[at] = pick_v[:, wide:]

    ga = [Gather(net, six(pka), True), Gather(net, six(pva), False)]
    gb = [Gather(net, six(pkb), True), Gather(net, six(pvb), False)]

    def each(gs, name, *j):
        for g in gs:
            getattr(g, name)(*j)

    each(ga, "phase0")
    units(3, 5)
    for a in tys:
        a.wait_recv()
    tzs = [net.copy(tab.at[c, z], tab.at[c, z], kv_of((z + d) % 4, y, c)) for d in range(1, 4)]
    each(ga, "phase1")
    units(5, 6)
    each(ga, "phase2")
    each(gb, "phase0")
    for a in tzs:
        a.wait_recv()
    tside = net.copy(tab.at[c], tab.at[c], partner)
    units(6, 7)
    each(ga, "phase3", 0)
    each(ga, "phase3", 1)
    each(gb, "phase1")
    units(7, 8)
    own_x = disk.copy(x_hbm, kb)
    tside.wait_recv()
    for i in range(32):
        spots[i:i + 1] = tab[i // 16, i // 4 % 4, i % 4, 0:1]
    disk.copy(spots, spots_s).wait()

    def owner_of(p):
        o = p // CAP
        return o, o % 16 * 2 + o // 16

    def tally(p, sums):
        o, kvi = owner_of(p)
        v = spots_s[o, p % CAP]
        live = (v >= 0) & (kvi < me)
        return tuple(t + jnp.where(live & (v // blocks == s), 1, 0) for s, t in enumerate(sums))

    zero = jnp.int32(0)
    sums = lax.fori_loop(0, slots, tally, (zero,) * 4)
    chunks = [(t + 3) // 4 for t in sums]
    base = [zero]
    for s in range(3):
        base.append(base[-1] + chunks[s])

    def arrange(p, state):
        heads_at, l_slot, l_id = state
        o, kvi = owner_of(p)
        v = spots_s[o, p % CAP]
        live = (v >= 0) & (kvi < me)
        to = jnp.int32(4 * room)
        now = []
        for s, t in enumerate(heads_at):
            hit = live & (v // blocks == s)
            to = jnp.where(hit, t, to)
            now.append(t + jnp.where(hit, 1, 0))
        to_s[0, p] = to
        here = lane8 == to
        return tuple(now), jnp.where(here, p, l_slot), jnp.where(here, kvi * blocks + v % blocks, l_id)

    blank = jnp.zeros((8, 128), jnp.int32)
    _, l_slot, l_id = lax.fori_loop(
        0, slots, arrange, (tuple(4 * b for b in base), blank, blank - 5))
    row8 = lax.broadcasted_iota(jnp.int32, (8, 128), 0)
    info[...] = jnp.where(row8 == 0, l_slot, l_id)
    to_info = disk.copy(info, info_s)
    gk[4 * room] = jnp.zeros(gk.shape[1:], gk.dtype)
    gv[4 * room] = jnp.zeros(gv.shape[1:], gv.dtype)
    to_info.wait()
    count_me = jnp.where(me == 0, 0, (2 * me + 12) // 4)

    def seq_of(i):
        return sum(jnp.where(i >= base[s], 1, 0) for s in range(1, 4))

    each(ga, "phase3", 2)
    each(ga, "phase3", 3)
    each(gb, "phase2")
    for j in range(4):
        each(ga, "phase4", j)
    each(ga, "phase5")

    def attend(second):
        pk, pv = (pkb, pvb) if second else (pka, pva)

        def chunk(i, _):
            s = seq_of(i)
            keep = jnp.where((s == seq_of(i - 1)) & (i > 0), 1, 0)
            keep = jnp.broadcast_to(keep, (1, n)) == 1
            who = [(jnp.clip(info_s[0, 4 * i + e], 0, slots - 1), info_s[1, 4 * i + e]) for e in range(4)]
            for g in range(2):
                h = 2 * second + g
                gs = slice(g * DH, (g + 1) * DH)
                hs = slice(h * DH, (h + 1) * DH)
                q = qb[s, :, hs]
                do = dob[s, :, hs]
                k = jnp.concatenate([pk[o, :, gs] for o, _ in who], axis=0)
                v = jnp.concatenate([pv[o, :, gs] for o, _ in who], axis=0)
                lse = lse_ref[s, h:h + 1, :]
                st = mm(k, q, NT)
                bias = jnp.concatenate(
                    [jnp.broadcast_to(bias_row(lse, s, b), (BLK, n)) for _, b in who], axis=0)
                p = jnp.exp2(st * (ROOT * LOG2E) - bias)
                dp = mm(v, do, NT)
                ds = (p * (dp - delta_ref[s, h:h + 1, :])).astype(jnp.bfloat16)
                dv = mm(p.astype(jnp.bfloat16), do, NN).astype(jnp.bfloat16)
                dk = (mm(ds, q, NN) * ROOT).astype(jnp.bfloat16)
                for e in range(4):
                    gv[4 * i + e, :, gs] = dv[e * BLK:(e + 1) * BLK]
                    gk[4 * i + e, :, gs] = dk[e * BLK:(e + 1) * BLK]
                old = part[2 * jnp.maximum(i - 1, 0) + g]
                part[2 * i + g] = jnp.where(keep, old, 0.0) + mm(k, ds, TN)
            return 0

        return lambda a, b: lax.fori_loop(jnp.minimum(a, count_me), jnp.minimum(b, count_me), chunk, 0)

    def settle(second):
        pk, pv = (pkb, pvb) if second else (pka, pva)

        def move(o, _):
            for b in range(CAP):
                to = jnp.clip(to_s[0, o * CAP + b], 0, 4 * room)
                pk[o * CAP + b] = gk[to]
                pv[o * CAP + b] = gv[to]
            return 0

        lax.fori_loop(0, 32, move, 0)

    def queries(second):
        for s in range(seqs):
            end = jnp.clip(base[s] + chunks[s] - 1, 0, room - 1)
            for g in range(2):
                h = 2 * second + g
                hs = slice(h * DH, (h + 1) * DH)
                more = jnp.where(jnp.broadcast_to(chunks[s], (1, n)) > 0, part[2 * end + g], 0.0)
                dqb[s, :, :, hs] = ((dqt[s, hs, :] + more).T * ROOT).astype(jnp.bfloat16).reshape(-1, BLK, DH)

    def side(buf, into):
        return net.copy(six(buf).at[1 - c], into, partner)

    def fold(buf, into, copy):
        copy.wait_recv()

        def add(i, _):
            at = c * 32 + i
            a = buf[at].astype(jnp.float32)
            buf[at] = (a + into[i // 8, i // 2 % 4, i % 2].astype(jnp.float32)).astype(jnp.bfloat16)
            return 0

        lax.fori_loop(0, 32, add, 0)

    first_half = attend(0)
    first_half(0, 3)
    each(gb, "phase3", 0)
    each(gb, "phase3", 1)
    first_half(3, 6)
    each(gb, "phase3", 2)
    each(gb, "phase3", 3)
    first_half(6, 9)
    for j in range(4):
        each(gb, "phase4", j)
    x.pass_on(0)
    first_half(9, room)
    each(gb, "phase5")
    each(ga, "drain")
    settle(0)
    side_va = side(pva, rva)
    side_ka = side(pka, rka)
    queries(0)
    va = Stream(net, six(pva).at[c], vas)
    ka = Stream(net, six(pka).at[c], kas)
    second_half = attend(1)
    fold(pva, rva, side_va)
    va.run("step1")
    second_half(0, 2)
    fold(pka, rka, side_ka)
    ka.run("step1")
    second_half(2, 6)
    va.run("step2")
    x.pass_on(1)
    second_half(6, 10)
    ka.run("step2")
    second_half(10, 14)
    va.run("step3")
    second_half(14, room)
    each(gb, "drain")
    settle(1)
    side_vb = side(pvb, rvb)
    side_kb = side(pkb, rkb)
    va.run("step4")
    ka.run("step3")
    queries(1)
    dq_out = disk.copy(dqb, dq_hbm)
    vsb = Stream(net, six(pvb).at[c], vbs)
    ksb = Stream(net, six(pkb).at[c], kbs)
    fold(pvb, rvb, side_vb)
    vsb.run("step1")
    fold(pkb, rkb, side_kb)
    ksb.run("step1")
    ka.run("step4")

    x.near()
    load_x = [own_x, disk.copy(xall_hbm.at[x.t[1]], vb), disk.copy(xall_hbm.at[x.t[2]], ob)]
    bufs = [kb, vb, ob, dqb]

    def product(i):
        load_x[i].wait()

        def step(s, _):
            r = mm(bufs[i][s].reshape(n, ch), dvb[s].reshape(n, ch), TN)
            for j in range(4):
                at = x.t[i] * 4 + j
                part[at] = part[at] + r[j * 128:(j + 1) * 128]
            return 0

        r = mm(bufs[i][0].reshape(n, ch), dvb[0].reshape(n, ch), TN)
        for j in range(4):
            part[x.t[i] * 4 + j] = r[j * 128:(j + 1) * 128]
        lax.fori_loop(1, seqs, step, 0)

    product(0)
    vsb.run("step2")
    fva = va.run("step5")
    product(1)
    ksb.run("step2")
    fka = ka.run("step5")
    vsb.run("step3")
    product(2)
    vsb.run("step4")
    x.far()
    dq_out.wait()
    load_x.append(disk.copy(xall_hbm.at[x.t[3]], dqb))
    product(3)
    old = jnp.concatenate(rows_of(dvb), axis=0).astype(jnp.float32)
    xs = [jnp.concatenate(rows_of(b), axis=0) for b in bufs]
    fvb = vsb.run("step5")

    def joined(a, b):
        return jnp.concatenate([jnp.concatenate(a, axis=0), jnp.concatenate(b, axis=0)], axis=1)

    extra_v = joined(fva, fvb)
    diff = ((old + extra_v).astype(jnp.bfloat16).astype(jnp.float32) - old).astype(jnp.bfloat16)
    mine, other = pl.multiple_of(c * BLK, BLK), pl.multiple_of((1 - c) * BLK, BLK)
    for i in range(4):
        r = mm(xs[i], diff, TN)
        for j in range(4):
            at = x.t[i] * 4 + j
            part[at] = part[at] + r[j * 128:(j + 1) * 128]
            ws[at] = part[at, pl.ds(other, BLK)].astype(jnp.bfloat16)
    side_w = net.copy(ws, wr, partner)
    ksb.run("step3")
    side_w.wait_recv()
    for i in range(16):
        own = part[i, pl.ds(mine, BLK)]
        wb[i // 4, i % 4] = (own + wr[i].astype(jnp.float32)).astype(jnp.bfloat16).reshape(2, BLK // 2, ch)
    w = Stream(net, wb, wslots)
    w.run("step1")
    ksb.run("step4")

    def finish(local_ref, extra):
        def add(i, _):
            at = (i // blocks, i % blocks)
            more = jnp.where(served0 == i, extra[:BLK], 0.0) + jnp.where(served1 == i, extra[BLK:], 0.0)
            local_ref[at] = (local_ref[at].astype(jnp.float32) + more).astype(jnp.bfloat16)
            return 0

        lax.fori_loop(0, seqs * blocks, add, 0)

    w.run("step2")
    finish(dvb, extra_v)
    disk.keep(dvb, dv_hbm)
    fkb = ksb.run("step5")
    w.run("step3")
    finish(dkb, joined(fka, fkb))
    disk.keep(dkb, dk_hbm)
    w.run("step4")
    top, low = w.run("step5")
    dw_ref[:BLK // 2] = top
    dw_ref[BLK // 2:] = low
    done = set(id(a) for g in ga + gb for a in g.sent)
    for a in net.all:
        if id(a) not in done:
            a.wait_send()
    disk.finish()


def fused(code, lse, pick, q, k, v, o, do, x):
    seqs, n, ch = q.shape
    blk = k.shape
    heads = ch // DH
    bf, f32, i32 = jnp.bfloat16, jnp.float32, jnp.int32
    wide = ch // 2
    whole = pl.BlockSpec(memory_space=pltpu.VMEM)
    hbm = pl.BlockSpec(memory_space=pl.ANY)
    V = pltpu.VMEM
    return pl.pallas_call(
        whole_kernel,
        in_specs=[pl.BlockSpec(memory_space=pltpu.SMEM)] + [whole] * 2 + [hbm] * 6,
        out_specs=[hbm] * 3 + [whole, hbm],
        out_shape=[
            jax.ShapeDtypeStruct(blk, bf),
            jax.ShapeDtypeStruct(blk, bf),
            jax.ShapeDtypeStruct(blk, bf),
            jax.ShapeDtypeStruct((BLK, ch), f32),
            jax.ShapeDtypeStruct((4,) + x.shape, bf),
        ],
        scratch_shapes=[V(q.shape, bf)] + [V(blk, bf)] * 3 + [V(q.shape, bf), V((seqs, ch, n), f32)] + [V(blk, bf)] * 3 + [
            V((seqs, heads, n), f32),
            V((2, 4, 4, 8, 128), i32), V((4, 4, 8, 128), i32), V((4, 4, 8, 128), i32),
            V((3, 4, 8, 128), i32), V((4, 8, 128), i32), V((3, 8, 128), i32), V((2, 4, 4, 8, 128), i32),
            V((64, BLK, wide), bf), V((64, BLK, wide), bf), V((64, BLK, wide), bf), V((64, BLK, wide), bf),
            V((73, BLK, wide), bf), V((73, BLK, wide), bf), V((36, DH, n), f32),
            V((8, 128), i32), V((32, 128), i32),
            pltpu.SMEM((8, 128), i32), pltpu.SMEM((32, 128), i32), pltpu.SMEM((8, 128), i32),
        ] + [V((4, 4, CAP, BLK, wide), bf)] * 4 + [
            V((16, BLK, ch), bf), V((16, BLK, ch), bf), V((4, 4, 2, BLK // 2, ch), bf),
        ] + (route_scratch(BLK, wide, bf) * 2 + route_scratch(BLK, wide, f32) * 2) * 2
        + route_scratch(BLK // 2, ch, f32) * 2 + [
            pltpu.SemaphoreType.DMA((256,)), pltpu.SemaphoreType.DMA((256,)), pltpu.SemaphoreType.DMA((20,)),
        ],
        compiler_params=pltpu.CompilerParams(
            vmem_limit_bytes=67043328, collective_id=0, has_side_effects=True),
        cost_estimate=pl.CostEstimate(flops=20_000_000_000, bytes_accessed=30 << 20, transcendentals=1 << 22),
        name="fused_backward",
    )(code, lse, pick, q, k, v, o, do, x)


def body(layer_input, queries, keys, values, outputs, d_out, log_sums, chosen):
    seqs, n, ch = queries.shape
    blocks = n // BLK
    me = lax.axis_index("kv")
    lse = jnp.swapaxes(log_sums, 1, 2) * LOG2E
    owner = chosen // blocks
    row = (owner % 2) * 16 + (owner // 2 % 4) * 4 + owner // 8
    lane = jnp.arange(seqs, dtype=jnp.int32)[:, None, None] * blocks + chosen % blocks
    code = jnp.where((chosen >= 0) & (owner != me), row * 128 + lane, -1).reshape(-1)
    pick = jnp.swapaxes(chosen, 1, 2)
    pick = jnp.pad(pick, ((0, 0), (0, 16 - pick.shape[1]), (0, 0)), constant_values=-1)
    pick = jnp.repeat(pick, BLK, axis=2)

    def cut(a):
        return a.reshape(seqs, blocks, BLK, ch)

    dq, dk, dv, dw, _ = fused(code, lse, pick, queries, cut(keys), cut(values), cut(outputs), d_out, cut(layer_input))
    return dq.reshape(queries.shape), dk.reshape(queries.shape), dv.reshape(queries.shape), dw


def solution(mesh):
    spec = P(None, "kv", "tp")
    return jax.shard_map(
        body,
        mesh=mesh,
        in_specs=(spec,) * 7 + (P(None, "kv", None),),
        out_specs=(spec, spec, spec, P("kv", "tp")),
        check_vma=False,
    )
```

```python
import functools
import jax
import jax.numpy as jnp
from jax import lax
from jax.experimental import pallas as pl
from jax.experimental.pallas import tpu as pltpu
from jax.sharding import PartitionSpec as P

BLK = 64
CAP = 2
DH = 128
LOG2E = 1.4426950408889634
ROOT = DH ** -0.5
BIG = 1e30

NT = (((1,), (1,)), ((), ()))
TN = (((0,), (0,)), ((), ()))
NN = (((1,), (0,)), ((), ()))


def mm(a, b, dims):
    return lax.dot_general(a, b, dims, preferred_element_type=jnp.float32)


class Net:
    def __init__(self, send, recv):
        self.send, self.recv, self.n, self.ns, self.all = send, recv, 0, 0, []

    def new_send(self):
        self.ns += 1
        return self.ns - 1

    def new_recv(self):
        self.n += 1
        return self.n - 1

    def copy(self, src, dst, kv, tp=None, ss=None, rs=None):
        shared = ss is not None
        ss = self.new_send() if ss is None else ss
        rs = self.new_recv() if rs is None else rs
        c = self.make(src, dst, kv, tp, ss, rs)
        c.start()
        if not shared:
            self.all.append(c)
        return c

    def make(self, src, dst, kv, tp, ss, rs):
        return pltpu.make_async_remote_copy(
            src_ref=src, dst_ref=dst, send_sem=self.send.at[ss], recv_sem=self.recv.at[rs],
            device_id=(kv, lax.axis_index("tp") if tp is None else tp), device_id_type=pl.DeviceIdType.MESH)

    def wait_recv(self, ref, rs):
        self.make(ref, ref, (lax.axis_index("kv") + 1) % 32, None, 0, rs).wait_recv()

    def wait_send(self, ref, ss):
        self.make(ref, ref, (lax.axis_index("kv") + 1) % 32, None, ss, 0).wait_send()

    def finish(self):
        for c in self.all:
            c.wait_send()


class Disk:
    def __init__(self, sems):
        self.sems, self.n, self.all = sems, 0, []

    def copy(self, src, dst):
        c = pltpu.make_async_copy(src, dst, self.sems.at[self.n])
        self.n += 1
        c.start()
        return c

    def keep(self, src, dst):
        self.all.append(self.copy(src, dst))

    def finish(self):
        for c in self.all:
            c.wait()


def place():
    me = lax.axis_index("kv")
    return me // 8, (me // 2) % 4, me % 2


def kv_of(z, y, c):
    return (z * 4 + y) * 2 + c


def greet(peers, across):
    sem = pltpu.get_barrier_semaphore()
    for kv in peers:
        pl.semaphore_signal(sem, inc=1, device_id=(kv, lax.axis_index("tp")),
                            device_id_type=pl.DeviceIdType.MESH)
    for tp in across:
        pl.semaphore_signal(sem, inc=1, device_id=(lax.axis_index("kv"), tp),
                            device_id_type=pl.DeviceIdType.MESH)


SENDS, RECVS = 38, 189


class Gather:
    def __init__(self, net, buf, y_first):
        z, y, c = place()
        self.net, self.buf, self.y_first = net, buf, y_first
        f, s = (y, z) if y_first else (z, y)
        self.c = c
        self.f = [f, (f + 3) % 4, (f + 1) % 4, (f + 2) % 4]
        self.s = [s, (s + 3) % 4, (s + 1) % 4, (s + 2) % 4]
        self.out, self.away, self.near = net.new_send(), net.new_send(), net.new_recv()

    def full(self, f, s, c=None):
        c = self.c if c is None else c
        return self.buf.at[(c, s, f) if self.y_first else (c, f, s)]

    def half(self, f, s, which):
        c = self.c
        return self.buf.at[(c, s, f, which) if self.y_first else (c, f, s, which)]

    def send(self, ref, f, s, c=None, near=False):
        c = self.c if c is None else c
        kv = kv_of(s, f, c) if self.y_first else kv_of(f, s, c)
        if near:
            return self.net.copy(ref, ref, kv, ss=self.away, rs=self.near)
        return self.net.copy(ref, ref, kv, ss=self.out)

    def have(self, f, s):
        self.send(self.full(f, s), self.f[0], self.s[0], 1 - self.c, True)

    def across(self, f):
        return (self.send(self.full(f, self.s[0]), self.f[0], self.s[2]),
                self.send(self.full(f, self.s[0]), self.f[0], self.s[1]))

    def phase0(self):
        own = self.full(self.f[0], self.s[0])
        self.a = self.send(own, self.f[2], self.s[0])
        self.b = self.send(own, self.f[1], self.s[0])
        self.second = [self.across(self.f[0])]
        self.have(self.f[0], self.s[0])

    def phase1(self):
        self.a.wait_recv()
        self.e = self.send(self.half(self.f[1], self.s[0], 0), self.f[2], self.s[0])
        self.second.append(self.across(self.f[1]))
        self.b.wait_recv()
        self.g = self.send(self.half(self.f[2], self.s[0], 1), self.f[1], self.s[0])
        self.second.append(self.across(self.f[2]))
        self.have(self.f[1], self.s[0])
        self.have(self.f[2], self.s[0])

    def phase2(self):
        self.e.wait_recv()
        self.g.wait_recv()
        self.second.append(self.across(self.f[3]))
        self.have(self.f[3], self.s[0])
        self.last = []

    def phase3(self, j):
        up, down = self.second[j]
        up.wait_recv()
        p = self.send(self.half(self.f[j], self.s[1], 0), self.f[0], self.s[2])
        down.wait_recv()
        q = self.send(self.half(self.f[j], self.s[2], 1), self.f[0], self.s[1])
        self.last.append((p, q))
        self.have(self.f[j], self.s[1])
        self.have(self.f[j], self.s[2])

    def phase4(self, j):
        for c in self.last[j]:
            c.wait_recv()
        self.have(self.f[j], self.s[3])

    def phase5(self):
        self.net.wait_recv(self.buf.at[1 - self.c], self.near)

    def drain(self, flat):
        self.net.wait_send(self.buf.at[self.c], self.away)
        self.net.wait_send(flat.at[pl.ds(0, 30)], self.out)


class Route:
    def __init__(self, net, buf, rows, y_first, slots, out):
        z, y, c = place()
        self.net, self.buf, self.rows, self.y_first, self.out = net, buf, rows, y_first, out
        self.ra, self.rb, self.rp, self.rm, self.e, self.ta, self.tb, self.tp, self.tm = slots
        self.c = c
        self.f, self.s = (y, z) if y_first else (z, y)
        self.wide = buf.shape[-1] // 2
        self.kind = self.e.dtype

    def dev(self, f, s):
        return kv_of(s, f, self.c) if self.y_first else kv_of(f, s, self.c)

    def src(self, f, part=None):
        lanes = pl.ds(0, 2 * self.wide) if part is None else pl.ds(part * self.wide, self.wide)
        if self.y_first:
            return self.buf.at[:, f, self.rows, :, lanes]
        return self.buf.at[f, :, self.rows, :, lanes]

    def step1(self):
        f, s = self.f, self.s
        self.c1 = (self.net.copy(self.src((f + 2) % 4, 0), self.ra, self.dev((f + 1) % 4, s), ss=self.out),
                   self.net.copy(self.src((f + 2) % 4, 1), self.rb, self.dev((f + 3) % 4, s), ss=self.out))

    def step2(self):
        f, s, w = self.f, self.s, self.wide
        self.c2 = []
        for i, (d, got, dst) in enumerate(((1, self.ra, self.rp), (3, self.rb, self.rm))):
            self.c1[i].wait_recv()
            at = self.src((f + d) % 4, i)
            at[...] = (at[...].astype(jnp.float32) + got[...].astype(jnp.float32)).astype(jnp.bfloat16)
            self.c2.append(self.net.copy(self.src((f + d) % 4), dst, self.dev((f + d) % 4, s), ss=self.out))

    def step3(self):
        f, s, w = self.f, self.s, self.wide
        for x in self.c2:
            x.wait_recv()
        total = self.src(f)[...].astype(jnp.float32) + self.rp[...].astype(jnp.float32)
        self.e[...] = (total + self.rm[...].astype(jnp.float32)).astype(self.kind)
        far = (s + 2) % 4
        self.c3 = (self.net.copy(self.e.at[far, :, pl.ds(0, w)], self.ta, self.dev(f, (s + 1) % 4), ss=self.out),
                   self.net.copy(self.e.at[far, :, pl.ds(w, w)], self.tb, self.dev(f, (s + 3) % 4), ss=self.out))

    def step4(self):
        f, s, w = self.f, self.s, self.wide
        self.c4 = []
        for i, (d, got, dst) in enumerate(((1, self.ta, self.tp), (3, self.tb, self.tm))):
            self.c3[i].wait_recv()
            at = self.e.at[(s + d) % 4, :, pl.ds(i * w, w)]
            at[...] = (at[...].astype(jnp.float32) + got[...].astype(jnp.float32)).astype(self.kind)
            self.c4.append(self.net.copy(self.e.at[(s + d) % 4], dst, self.dev(f, (s + d) % 4), ss=self.out))

    def step5(self):
        for x in self.c4:
            x.wait_recv()
        total = self.e[self.s].astype(jnp.float32) + self.tp[...].astype(jnp.float32)
        return total + self.tm[...].astype(jnp.float32)


def route_scratch(rows, ch, kind):
    bf = jnp.bfloat16
    return [pltpu.VMEM((4, rows, ch // 2), bf), pltpu.VMEM((4, rows, ch // 2), bf),
            pltpu.VMEM((4, rows, ch), bf), pltpu.VMEM((4, rows, ch), bf), pltpu.VMEM((4, rows, ch), kind),
            pltpu.VMEM((rows, ch // 2), kind), pltpu.VMEM((rows, ch // 2), kind),
            pltpu.VMEM((rows, ch), kind), pltpu.VMEM((rows, ch), kind)]


class Stream:
    def __init__(self, net, buf, slots):
        self.net, self.out = net, net.new_send()
        self.blocks = 36 if slots[4].dtype == jnp.float32 else 30
        self.routes = [Route(net, buf, 0, True, slots[:9], self.out), Route(net, buf, 1, False, slots[9:], self.out)]

    def drain(self, flat):
        self.net.wait_send(flat.at[pl.ds(0, self.blocks)], self.out)

    def run(self, name):
        return [getattr(r, name)() for r in self.routes]


class Ring:
    def __init__(self, net, own, everyone):
        self.net, self.own, self.all = net, own, everyone
        t = lax.axis_index("tp")
        self.t = [t, (t + 3) % 4, (t + 1) % 4, (t + 2) % 4]
        self.onward = []

    def start(self):
        t = self.t
        self.up, self.down = [], []
        for j in range(4):
            self.up.append(self.copy(self.own.at[j], self.all.at[t[0], j], t[2]))
            i = (j + 2) % 4
            self.down.append(self.copy(self.own.at[i], self.all.at[t[0], i], t[1]))

    def copy(self, src, dst, tp):
        return self.net.copy(src, dst, lax.axis_index("kv"), tp)

    def pass_on(self, j):
        self.up[j].wait_recv()
        at = self.all.at[self.t[1], j]
        self.onward.append(self.copy(at, at, self.t[2]))
        self.down[j].wait_recv()
        at = self.all.at[self.t[2], j + 2]
        self.onward.append(self.copy(at, at, self.t[1]))

    def near(self):
        for c in self.up[2:] + self.down[2:]:
            c.wait_recv()

    def far(self):
        for c in self.onward:
            c.wait_recv()


def whole_kernel(chosen_ref, sums_ref, q_hbm, k_hbm, v_hbm, o_hbm, do_hbm, x_hbm,
                 dq_hbm, dk_hbm, dv_hbm, dw_ref, xall_hbm,
                 qb, kb, vb, ob, dob, dqt, dkb, dvb, dqb, delta_ref,
                 need, names, lse_ref, pick_ref, square, codes, codes_s, tab, pka, pva, pkb, pvb, gk, gv, part,
                 info, spots, info_s, spots_s, to_s, rka, rva, rkb, rvb, ws, wr, wb, *rest):
    kas, vas, kbs, vbs, wslots = (rest[i * 18:i * 18 + 18] for i in range(5))
    send, recv, local = rest[90:]
    z, y, c = place()
    me = lax.axis_index("kv")
    net, disk = Net(send, recv), Disk(local)
    loads = [disk.copy(a, b) for a, b in
             ((k_hbm, kb), (v_hbm, vb), (q_hbm, qb), (do_hbm, dob), (o_hbm, ob))]
    partner = kv_of(z, y, 1 - c)
    peers = [(me + d) % 32 for d in range(1, 32)]
    x = Ring(net, x_hbm, xall_hbm)
    greet(peers, x.t[1:3])
    seqs, n, ch = qb.shape
    half = n // 2

    def six(ref):
        return ref.reshape(2, 4, 4, CAP, BLK, ch // 2)

    blocks = n // BLK
    wide = ch // 2
    slots = 32 * CAP
    room = 18

    for t in range(seqs):
        v = chosen_ref[t]
        there = v >> 3
        codes[t, :, :12] = jnp.where((v >= 0) & (there != me), there * 128 + t * blocks + (v & 7), -1)
    to_codes = disk.copy(codes, codes_s)
    lse_ref[...] = sums_ref[...] * LOG2E
    rep_rows = lax.broadcasted_iota(jnp.int32, (128, n), 0)
    rep_cols = lax.broadcasted_iota(jnp.int32, (128, n), 1)
    stretch = jnp.where(rep_rows == rep_cols // BLK, 1.0, 0.0).astype(jnp.bfloat16)
    for t in range(seqs):
        square[...] = jnp.full((128, 128), -1.0, jnp.float32)
        square[:8, :12] = chosen_ref[t].astype(jnp.float32)
        pick_ref[t] = mm(square[...].astype(jnp.bfloat16), stretch, TN)[:16]
    flat = (lax.broadcasted_iota(jnp.int32, (32, 128), 0) * 128 +
            lax.broadcasted_iota(jnp.int32, (32, 128), 1))
    to_codes.wait()

    def mark(i, seen):
        for j in range(12):
            seen = jnp.where(flat == codes_s[i // 8, i % 8, j], 1, seen)
        return seen

    seen = lax.fori_loop(0, 32, mark, jnp.zeros((32, 128), jnp.int32))
    for i in range(32):
        need[i] = seen[i:i + 1]
    pl.semaphore_wait(pltpu.get_barrier_semaphore(), len(peers) + 2)
    told, heard = net.new_send(), net.new_recv()
    for d in range(1, 32):
        to = (me + d) % 32
        net.copy(need.at[to], names.at[me], to, ss=told, rs=heard)
    names[me] = jnp.zeros((1, 128), jnp.int32)
    x.start()
    for l in loads:
        l.wait()

    def bias_row(lse, s, block):
        hit = jnp.max(jnp.where(pick_ref[s] == jnp.asarray(block, jnp.float32), 1.0, 0.0), axis=0, keepdims=True)
        return jnp.where(hit > 0.5, lse, BIG)

    def unit(u, _):
        s = u // 2
        for g in range(2):
            h = (u % 2) * 2 + g
            hs = pl.ds(pl.multiple_of(h * DH, DH), DH)
            hr = pl.ds(h, 1)
            q = qb[s, :, hs]
            do = dob[s, :, hs]
            prod = do.astype(jnp.float32) * ob[s, :, :, hs].reshape(n, DH).astype(jnp.float32)
            delta = jnp.sum(prod.T, axis=0, keepdims=True)
            delta_ref[s, hr, :] = delta
            lse = lse_ref[s, hr, :]
            parts = []
            for t in range(2):
                lo = t * half
                here = slice(lo // BLK, (lo + half) // BLK)
                k = kb[s, here, :, hs].reshape(half, DH)
                v = vb[s, here, :, hs].reshape(half, DH)
                qc, doc = q[lo:], do[lo:]
                w = n - lo
                sc = mm(k, qc, NT)
                row = lax.broadcasted_iota(jnp.int32, (half, w), 0)
                col = lax.broadcasted_iota(jnp.int32, (half, w), 1)
                bias = jnp.concatenate(
                    [jnp.broadcast_to(bias_row(lse, s, me * blocks + j)[:, lo:], (BLK, w))
                     for j in range(lo // BLK, (lo + half) // BLK)], axis=0)
                p = jnp.exp2(jnp.where(row <= col, sc * (ROOT * LOG2E) - bias, -BIG))
                dp = mm(v, doc, NT)
                ds = (p * (dp - delta[:, lo:])).astype(jnp.bfloat16)
                dvb[s, here, :, hs] = mm(p.astype(jnp.bfloat16), doc, NN).astype(jnp.bfloat16).reshape(-1, BLK, DH)
                dkb[s, here, :, hs] = (mm(ds, qc, NN) * ROOT).astype(jnp.bfloat16).reshape(-1, BLK, DH)
                parts.append(mm(k, ds, TN))
            dqt[s, hs, :half] = parts[0][:, :half]
            dqt[s, hs, half:] = parts[0][:, half:] + parts[1]
        return 0

    def units(a, b):
        lax.fori_loop(a, b, unit, 0)

    units(0, 1)
    net.wait_recv(names.at[pl.ds(0, 31)], heard)
    need1 = jnp.broadcast_to(jnp.max(names[...], axis=0), (8, 128))
    info[...] = need1
    disk.copy(info, info_s).wait()

    def first_two(i, state):
        seen, s0, s1 = state
        here = info_s[0, i]
        s0 = jnp.where((here == 1) & (seen == 0), i, s0)
        s1 = jnp.where((here == 1) & (seen == 1), i, s1)
        return seen + here, s0, s1

    minus = jnp.int32(-1)
    _, served0, served1 = lax.fori_loop(0, seqs * blocks, first_two, (jnp.int32(0), minus, minus))
    served = (served0, served1)
    lane8 = lax.broadcasted_iota(jnp.int32, (8, 128), 1)
    tab[c, z, y] = jnp.where(lane8 == 0, served0, jnp.where(lane8 == 1, served1, minus))
    tys = [net.copy(tab.at[c, z, y], tab.at[c, z, y], kv_of(z, (y + d) % 4, c)) for d in range(1, 4)]

    def rows_of(ref):
        out = []
        for b in served:
            b = jnp.clip(b, 0, seqs * blocks - 1)
            out.append(ref[b // blocks, b % blocks])
        return out

    for b, (pick_k, pick_v) in enumerate(zip(rows_of(kb), rows_of(vb))):
        at = (c * 16 + z * 4 + y) * CAP + b
        pka[at] = pick_k[:, :wide]
        pva[at] = pick_v[:, :wide]
        pkb[at] = pick_k[:, wide:]
        pvb[at] = pick_v[:, wide:]

    ga = [Gather(net, six(pka), True), Gather(net, six(pva), False)]
    gb = [Gather(net, six(pkb), True), Gather(net, six(pvb), False)]

    def each(gs, name, *j):
        for g in gs:
            getattr(g, name)(*j)

    each(ga, "phase0")
    units(1, 3)
    for a in tys:
        a.wait_recv()
    tzs = [net.copy(tab.at[c, z], tab.at[c, z], kv_of((z + d) % 4, y, c)) for d in range(1, 4)]
    each(ga, "phase1")
    units(3, 5)
    each(ga, "phase2")
    each(gb, "phase0")
    for a in tzs:
        a.wait_recv()
    tside = net.copy(tab.at[c], tab.at[c], partner)
    units(5, 7)
    each(ga, "phase3", 0)
    each(ga, "phase3", 1)
    each(gb, "phase1")
    units(7, 8)
    own_x = disk.copy(x_hbm, kb)
    tside.wait_recv()
    for i in range(32):
        spots[i:i + 1] = tab[i // 16, i // 4 % 4, i % 4, 0:1]
    disk.copy(spots, spots_s).wait()

    def owner_of(p):
        o = p // CAP
        return o, o % 16 * 2 + o // 16

    def tally(p, sums):
        o, kvi = owner_of(p)
        v = spots_s[o, p % CAP]
        live = (v >= 0) & (kvi < me)
        return tuple(t + jnp.where(live & (v // blocks == s), 1, 0) for s, t in enumerate(sums))

    zero = jnp.int32(0)
    sums = lax.fori_loop(0, slots, tally, (zero,) * 4)
    chunks = [(t + 3) // 4 for t in sums]
    base = [zero]
    for s in range(3):
        base.append(base[-1] + chunks[s])

    def arrange(p, state):
        heads_at, l_slot, l_id = state
        o, kvi = owner_of(p)
        v = spots_s[o, p % CAP]
        live = (v >= 0) & (kvi < me)
        to = jnp.int32(4 * room)
        now = []
        for s, t in enumerate(heads_at):
            hit = live & (v // blocks == s)
            to = jnp.where(hit, t, to)
            now.append(t + jnp.where(hit, 1, 0))
        to_s[0, p] = to
        here = lane8 == to
        return tuple(now), jnp.where(here, p, l_slot), jnp.where(here, kvi * blocks + v % blocks, l_id)

    blank = jnp.zeros((8, 128), jnp.int32)
    _, l_slot, l_id = lax.fori_loop(
        0, slots, arrange, (tuple(4 * b for b in base), blank, blank - 5))
    row8 = lax.broadcasted_iota(jnp.int32, (8, 128), 0)
    info[...] = jnp.where(row8 == 0, l_slot, l_id)
    to_info = disk.copy(info, info_s)
    gk[4 * room] = jnp.zeros(gk.shape[1:], gk.dtype)
    gv[4 * room] = jnp.zeros(gv.shape[1:], gv.dtype)
    to_info.wait()
    count_me = jnp.where(me == 0, 0, (2 * me + 12) // 4)

    def seq_of(i):
        return sum(jnp.where(i >= base[s], 1, 0) for s in range(1, 4))

    each(ga, "phase3", 2)
    each(ga, "phase3", 3)
    each(gb, "phase2")
    for j in range(4):
        each(ga, "phase4", j)
    each(ga, "phase5")

    def attend(second):
        pk, pv = (pkb, pvb) if second else (pka, pva)

        def chunk(i, _):
            s = seq_of(i)
            keep = jnp.where((s == seq_of(i - 1)) & (i > 0), 1, 0)
            keep = jnp.broadcast_to(keep, (1, n)) == 1
            who = [(jnp.clip(info_s[0, 4 * i + e], 0, slots - 1), info_s[1, 4 * i + e]) for e in range(4)]
            for g in range(2):
                h = 2 * second + g
                gs = slice(g * DH, (g + 1) * DH)
                hs = slice(h * DH, (h + 1) * DH)
                q = qb[s, :, hs]
                do = dob[s, :, hs]
                k = jnp.concatenate([pk[o, :, gs] for o, _ in who], axis=0)
                v = jnp.concatenate([pv[o, :, gs] for o, _ in who], axis=0)
                lse = lse_ref[s, h:h + 1, :]
                st = mm(k, q, NT)
                bias = jnp.concatenate(
                    [jnp.broadcast_to(bias_row(lse, s, b), (BLK, n)) for _, b in who], axis=0)
                p = jnp.exp2(st * (ROOT * LOG2E) - bias)
                dp = mm(v, do, NT)
                ds = (p * (dp - delta_ref[s, h:h + 1, :])).astype(jnp.bfloat16)
                dv = mm(p.astype(jnp.bfloat16), do, NN).astype(jnp.bfloat16)
                dk = (mm(ds, q, NN) * ROOT).astype(jnp.bfloat16)
                for e in range(4):
                    gv[4 * i + e, :, gs] = dv[e * BLK:(e + 1) * BLK]
                    gk[4 * i + e, :, gs] = dk[e * BLK:(e + 1) * BLK]
                old = part[2 * jnp.maximum(i - 1, 0) + g]
                part[2 * i + g] = jnp.where(keep, old, 0.0) + mm(k, ds, TN)
            return 0

        return lambda a, b: lax.fori_loop(jnp.minimum(a, count_me), jnp.minimum(b, count_me), chunk, 0)

    def settle(second):
        pk, pv = (pkb, pvb) if second else (pka, pva)

        def move(o, _):
            for b in range(CAP):
                to = jnp.clip(to_s[0, o * CAP + b], 0, 4 * room)
                pk[o * CAP + b] = gk[to]
                pv[o * CAP + b] = gv[to]
            return 0

        lax.fori_loop(0, 32, move, 0)

    def queries(second):
        for s in range(seqs):
            end = jnp.clip(base[s] + chunks[s] - 1, 0, room - 1)
            for g in range(2):
                h = 2 * second + g
                hs = slice(h * DH, (h + 1) * DH)
                more = jnp.where(jnp.broadcast_to(chunks[s], (1, n)) > 0, part[2 * end + g], 0.0)
                dqb[s, :, :, hs] = ((dqt[s, hs, :] + more).T * ROOT).astype(jnp.bfloat16).reshape(-1, BLK, DH)

    def side(buf, into):
        return net.copy(six(buf).at[1 - c], into, partner)

    def fold(buf, into, copy):
        copy.wait_recv()

        def add(i, _):
            at = c * 32 + i
            a = buf[at].astype(jnp.float32)
            buf[at] = (a + into[i // 8, i // 2 % 4, i % 2].astype(jnp.float32)).astype(jnp.bfloat16)
            return 0

        lax.fori_loop(0, 32, add, 0)

    first_half = attend(0)
    first_half(0, 3)
    each(gb, "phase3", 0)
    each(gb, "phase3", 1)
    first_half(3, 6)
    each(gb, "phase3", 2)
    each(gb, "phase3", 3)
    first_half(6, 9)
    for j in range(4):
        each(gb, "phase4", j)
    x.pass_on(0)
    first_half(9, room)
    each(gb, "phase5")
    ga[0].drain(pka)
    ga[1].drain(pva)
    settle(0)
    side_va = side(pva, rva)
    side_ka = side(pka, rka)
    queries(0)
    va = Stream(net, six(pva).at[c], vas)
    ka = Stream(net, six(pka).at[c], kas)
    second_half = attend(1)
    fold(pva, rva, side_va)
    va.run("step1")
    second_half(0, 2)
    fold(pka, rka, side_ka)
    ka.run("step1")
    second_half(2, 6)
    va.run("step2")
    x.pass_on(1)
    second_half(6, 10)
    ka.run("step2")
    second_half(10, 14)
    va.run("step3")
    second_half(14, room)
    gb[0].drain(pkb)
    gb[1].drain(pvb)
    settle(1)
    side_vb = side(pvb, rvb)
    side_kb = side(pkb, rkb)
    va.run("step4")
    ka.run("step3")
    queries(1)
    dq_out = disk.copy(dqb, dq_hbm)
    vsb = Stream(net, six(pvb).at[c], vbs)
    ksb = Stream(net, six(pkb).at[c], kbs)
    fold(pvb, rvb, side_vb)
    vsb.run("step1")
    ka.run("step4")
    fold(pkb, rkb, side_kb)

    x.near()
    load_x = [own_x, disk.copy(xall_hbm.at[x.t[1]], vb), disk.copy(xall_hbm.at[x.t[2]], ob)]
    bufs = [kb, vb, ob, dqb]

    def product(i):
        load_x[i].wait()

        def step(s, _):
            r = mm(bufs[i][s].reshape(n, ch), dvb[s].reshape(n, ch), TN)
            for j in range(4):
                at = x.t[i] * 4 + j
                part[at] = part[at] + r[j * 128:(j + 1) * 128]
            return 0

        r = mm(bufs[i][0].reshape(n, ch), dvb[0].reshape(n, ch), TN)
        for j in range(4):
            part[x.t[i] * 4 + j] = r[j * 128:(j + 1) * 128]
        lax.fori_loop(1, seqs, step, 0)

    product(0)
    vsb.run("step2")
    ksb.run("step1")
    fva = va.run("step5")
    product(1)
    fka = ka.run("step5")
    vsb.run("step3")
    product(2)
    vsb.run("step4")
    ksb.run("step2")
    x.far()
    dq_out.wait()
    load_x.append(disk.copy(xall_hbm.at[x.t[3]], dqb))
    product(3)
    old = jnp.concatenate(rows_of(dvb), axis=0).astype(jnp.float32)
    xs = [jnp.concatenate(rows_of(b), axis=0) for b in bufs]
    fvb = vsb.run("step5")

    def joined(a, b):
        return jnp.concatenate([jnp.concatenate(a, axis=0), jnp.concatenate(b, axis=0)], axis=1)

    extra_v = joined(fva, fvb)
    diff = ((old + extra_v).astype(jnp.bfloat16).astype(jnp.float32) - old).astype(jnp.bfloat16)
    mine, other = pl.multiple_of(c * BLK, BLK), pl.multiple_of((1 - c) * BLK, BLK)
    for i in range(4):
        r = mm(xs[i], diff, TN)
        for j in range(4):
            at = x.t[i] * 4 + j
            part[at] = part[at] + r[j * 128:(j + 1) * 128]
            ws[at] = part[at, pl.ds(other, BLK)].astype(jnp.bfloat16)
    side_w = net.copy(ws, wr, partner)
    ksb.run("step3")
    side_w.wait_recv()
    for i in range(16):
        own = part[i, pl.ds(mine, BLK)]
        wb[i // 4, i % 4] = (own + wr[i].astype(jnp.float32)).astype(jnp.bfloat16).reshape(2, BLK // 2, ch)
    w = Stream(net, wb, wslots)
    w.run("step1")
    ksb.run("step4")

    def finish(local_ref, extra):
        def add(i, _):
            at = (i // blocks, i % blocks)
            more = jnp.where(served0 == i, extra[:BLK], 0.0) + jnp.where(served1 == i, extra[BLK:], 0.0)
            local_ref[at] = (local_ref[at].astype(jnp.float32) + more).astype(jnp.bfloat16)
            return 0

        lax.fori_loop(0, seqs * blocks, add, 0)

    w.run("step2")
    finish(dvb, extra_v)
    disk.keep(dvb, dv_hbm)
    fkb = ksb.run("step5")
    w.run("step3")
    finish(dkb, joined(fka, fkb))
    disk.keep(dkb, dk_hbm)
    w.run("step4")
    top, low = w.run("step5")
    dw_ref[:BLK // 2] = top
    dw_ref[BLK // 2:] = low
    for st, ref in ((va, pva), (ka, pva), (vsb, pva), (ksb, pva), (w, pva)):
        st.drain(ref)
    net.wait_send(names.at[pl.ds(0, 31)], told)
    net.finish()
    disk.finish()
    assert net.n <= RECVS and net.ns <= SENDS, (net.n, net.ns)
    assert disk.n <= 16, disk.n


def fused(chosen, sums, q, k, v, o, do, x):
    seqs, n, ch = q.shape
    blk = k.shape
    heads = ch // DH
    bf, f32, i32 = jnp.bfloat16, jnp.float32, jnp.int32
    wide = ch // 2
    whole = pl.BlockSpec(memory_space=pltpu.VMEM)
    hbm = pl.BlockSpec(memory_space=pl.ANY)
    V = pltpu.VMEM
    return pl.pallas_call(
        whole_kernel,
        in_specs=[whole] * 2 + [hbm] * 6,
        out_specs=[hbm] * 3 + [whole, hbm],
        out_shape=[
            jax.ShapeDtypeStruct(blk, bf),
            jax.ShapeDtypeStruct(blk, bf),
            jax.ShapeDtypeStruct(blk, bf),
            jax.ShapeDtypeStruct((BLK, ch), f32),
            jax.ShapeDtypeStruct((4,) + x.shape, bf),
        ],
        scratch_shapes=[V(q.shape, bf)] + [V(blk, bf)] * 3 + [V(q.shape, bf), V((seqs, ch, n), f32)] + [V(blk, bf)] * 3 + [
            V((seqs, heads, n), f32),
            V((32, 1, 128), i32), V((32, 1, 128), i32), V((seqs, heads, n), f32), V((seqs, 16, n), f32),
            V((128, 128), f32), V((4, 8, 128), i32), pltpu.SMEM((4, 8, 128), i32), V((2, 4, 4, 8, 128), i32),
            V((64, BLK, wide), bf), V((64, BLK, wide), bf), V((64, BLK, wide), bf), V((64, BLK, wide), bf),
            V((73, BLK, wide), bf), V((73, BLK, wide), bf), V((36, DH, n), f32),
            V((8, 128), i32), V((32, 128), i32),
            pltpu.SMEM((8, 128), i32), pltpu.SMEM((32, 128), i32), pltpu.SMEM((8, 128), i32),
        ] + [V((4, 4, CAP, BLK, wide), bf)] * 4 + [
            V((16, BLK, ch), bf), V((16, BLK, ch), bf), V((4, 4, 2, BLK // 2, ch), bf),
        ] + (route_scratch(BLK, wide, bf) * 2 + route_scratch(BLK, wide, f32) * 2) * 2
        + route_scratch(BLK // 2, ch, f32) * 2 + [
            pltpu.SemaphoreType.DMA((SENDS,)), pltpu.SemaphoreType.DMA((RECVS,)), pltpu.SemaphoreType.DMA((16,)),
        ],
        compiler_params=pltpu.CompilerParams(
            vmem_limit_bytes=67043328, collective_id=0, has_side_effects=True),
        cost_estimate=pl.CostEstimate(flops=20_000_000_000, bytes_accessed=30 << 20, transcendentals=1 << 22),
        name="fused_backward",
    )(chosen, sums, q, k, v, o, do, x)


def body(layer_input, queries, keys, values, outputs, d_out, log_sums, chosen):
    seqs, n, ch = queries.shape
    blocks = n // BLK
    me = lax.axis_index("kv")
    def cut(a):
        return a.reshape(seqs, blocks, BLK, ch)

    dq, dk, dv, dw, _ = fused(chosen, jnp.swapaxes(log_sums, 1, 2), queries, cut(keys), cut(values),
                              cut(outputs), d_out, cut(layer_input))
    return tuple(jnp.where(me >= 0, a, jnp.zeros_like(a)).reshape(shape) for a, shape in
                 ((dq, queries.shape), (dk, queries.shape), (dv, queries.shape), (dw, dw.shape)))


def solution(mesh):
    spec = P(None, "kv", "tp")
    return jax.shard_map(
        body,
        mesh=mesh,
        in_specs=(spec,) * 7 + (P(None, "kv", None),),
        out_specs=(spec, spec, spec, P("kv", "tp")),
        check_vma=False,
    )
```

```python
import functools
import jax
import jax.numpy as jnp
from jax import lax
from jax.experimental import pallas as pl
from jax.experimental.pallas import tpu as pltpu
from jax.sharding import PartitionSpec as P

BLK = 64
CAP = 2
DH = 128
LOG2E = 1.4426950408889634
ROOT = DH ** -0.5
BIG = 1e30

NT = (((1,), (1,)), ((), ()))
TN = (((0,), (0,)), ((), ()))
NN = (((1,), (0,)), ((), ()))


def mm(a, b, dims):
    return lax.dot_general(a, b, dims, preferred_element_type=jnp.float32)


class Net:
    def __init__(self, send, recv):
        self.send, self.recv, self.n, self.ns, self.all = send, recv, 0, 0, []

    def new_send(self):
        self.ns += 1
        return self.ns - 1

    def new_recv(self):
        self.n += 1
        return self.n - 1

    def copy(self, src, dst, kv, tp=None, ss=None, rs=None):
        shared = ss is not None
        ss = self.new_send() if ss is None else ss
        rs = self.new_recv() if rs is None else rs
        c = self.make(src, dst, kv, tp, ss, rs)
        c.start()
        if not shared:
            self.all.append(c)
        return c

    def make(self, src, dst, kv, tp, ss, rs):
        return pltpu.make_async_remote_copy(
            src_ref=src, dst_ref=dst, send_sem=self.send.at[ss], recv_sem=self.recv.at[rs],
            device_id=(kv, lax.axis_index("tp") if tp is None else tp), device_id_type=pl.DeviceIdType.MESH)

    def wait_recv(self, ref, rs):
        self.make(ref, ref, (lax.axis_index("kv") + 1) % 32, None, 0, rs).wait_recv()

    def wait_send(self, ref, ss):
        self.make(ref, ref, (lax.axis_index("kv") + 1) % 32, None, ss, 0).wait_send()

    def finish(self):
        for c in self.all:
            c.wait_send()


class Disk:
    def __init__(self, sems):
        self.sems, self.n, self.all = sems, 0, []

    def copy(self, src, dst):
        c = pltpu.make_async_copy(src, dst, self.sems.at[self.n])
        self.n += 1
        c.start()
        return c

    def keep(self, src, dst):
        self.all.append(self.copy(src, dst))

    def finish(self):
        for c in self.all:
            c.wait()


def place():
    me = lax.axis_index("kv")
    return me // 8, (me // 2) % 4, me % 2


def kv_of(z, y, c):
    return (z * 4 + y) * 2 + c


def greet(peers, across):
    sem = pltpu.get_barrier_semaphore()
    for kv in peers:
        pl.semaphore_signal(sem, inc=1, device_id=(kv, lax.axis_index("tp")),
                            device_id_type=pl.DeviceIdType.MESH)
    for tp in across:
        pl.semaphore_signal(sem, inc=1, device_id=(lax.axis_index("kv"), tp),
                            device_id_type=pl.DeviceIdType.MESH)


SENDS, RECVS = 38, 189


class Gather:
    def __init__(self, net, buf, y_first):
        z, y, c = place()
        self.net, self.buf, self.y_first = net, buf, y_first
        f, s = (y, z) if y_first else (z, y)
        self.c = c
        self.f = [f, (f + 3) % 4, (f + 1) % 4, (f + 2) % 4]
        self.s = [s, (s + 3) % 4, (s + 1) % 4, (s + 2) % 4]
        self.out, self.away, self.near = net.new_send(), net.new_send(), net.new_recv()

    def full(self, f, s, c=None):
        c = self.c if c is None else c
        return self.buf.at[(c, s, f) if self.y_first else (c, f, s)]

    def half(self, f, s, which):
        c = self.c
        return self.buf.at[(c, s, f, which) if self.y_first else (c, f, s, which)]

    def send(self, ref, f, s, c=None, near=False):
        c = self.c if c is None else c
        kv = kv_of(s, f, c) if self.y_first else kv_of(f, s, c)
        if near:
            return self.net.copy(ref, ref, kv, ss=self.away, rs=self.near)
        return self.net.copy(ref, ref, kv, ss=self.out)

    def have(self, f, s):
        self.send(self.full(f, s), self.f[0], self.s[0], 1 - self.c, True)

    def across(self, f):
        return (self.send(self.full(f, self.s[0]), self.f[0], self.s[2]),
                self.send(self.full(f, self.s[0]), self.f[0], self.s[1]))

    def phase0(self):
        own = self.full(self.f[0], self.s[0])
        self.a = self.send(own, self.f[2], self.s[0])
        self.b = self.send(own, self.f[1], self.s[0])
        self.second = [self.across(self.f[0])]
        self.have(self.f[0], self.s[0])

    def phase1(self):
        self.a.wait_recv()
        self.e = self.send(self.half(self.f[1], self.s[0], 0), self.f[2], self.s[0])
        self.second.append(self.across(self.f[1]))
        self.b.wait_recv()
        self.g = self.send(self.half(self.f[2], self.s[0], 1), self.f[1], self.s[0])
        self.second.append(self.across(self.f[2]))
        self.have(self.f[1], self.s[0])
        self.have(self.f[2], self.s[0])

    def phase2(self):
        self.e.wait_recv()
        self.g.wait_recv()
        self.second.append(self.across(self.f[3]))
        self.have(self.f[3], self.s[0])
        self.last = []

    def phase3(self, j):
        up, down = self.second[j]
        up.wait_recv()
        p = self.send(self.half(self.f[j], self.s[1], 0), self.f[0], self.s[2])
        down.wait_recv()
        q = self.send(self.half(self.f[j], self.s[2], 1), self.f[0], self.s[1])
        self.last.append((p, q))
        self.have(self.f[j], self.s[1])
        self.have(self.f[j], self.s[2])

    def phase4(self, j):
        for c in self.last[j]:
            c.wait_recv()
        self.have(self.f[j], self.s[3])

    def phase5(self):
        self.net.wait_recv(self.buf.at[1 - self.c], self.near)

    def drain(self, flat):
        self.net.wait_send(self.buf.at[self.c], self.away)
        self.net.wait_send(flat.at[pl.ds(0, 30)], self.out)


class Route:
    def __init__(self, net, buf, rows, y_first, slots, out):
        z, y, c = place()
        self.net, self.buf, self.rows, self.y_first, self.out = net, buf, rows, y_first, out
        self.ra, self.rb, self.rp, self.rm, self.e, self.ta, self.tb, self.tp, self.tm = slots
        self.c = c
        self.f, self.s = (y, z) if y_first else (z, y)
        self.wide = buf.shape[-1] // 2
        self.kind = self.e.dtype

    def dev(self, f, s):
        return kv_of(s, f, self.c) if self.y_first else kv_of(f, s, self.c)

    def src(self, f, part=None):
        lanes = pl.ds(0, 2 * self.wide) if part is None else pl.ds(part * self.wide, self.wide)
        if self.y_first:
            return self.buf.at[:, f, self.rows, :, lanes]
        return self.buf.at[f, :, self.rows, :, lanes]

    def step1(self):
        f, s = self.f, self.s
        self.c1 = (self.net.copy(self.src((f + 2) % 4, 0), self.ra, self.dev((f + 1) % 4, s), ss=self.out),
                   self.net.copy(self.src((f + 2) % 4, 1), self.rb, self.dev((f + 3) % 4, s), ss=self.out))

    def step2(self):
        f, s, w = self.f, self.s, self.wide
        self.c2 = []
        for i, (d, got, dst) in enumerate(((1, self.ra, self.rp), (3, self.rb, self.rm))):
            self.c1[i].wait_recv()
            at = self.src((f + d) % 4, i)
            at[...] = (at[...].astype(jnp.float32) + got[...].astype(jnp.float32)).astype(jnp.bfloat16)
            self.c2.append(self.net.copy(self.src((f + d) % 4), dst, self.dev((f + d) % 4, s), ss=self.out))

    def step3(self):
        f, s, w = self.f, self.s, self.wide
        for x in self.c2:
            x.wait_recv()
        total = self.src(f)[...].astype(jnp.float32) + self.rp[...].astype(jnp.float32)
        self.e[...] = (total + self.rm[...].astype(jnp.float32)).astype(self.kind)
        far = (s + 2) % 4
        self.c3 = (self.net.copy(self.e.at[far, :, pl.ds(0, w)], self.ta, self.dev(f, (s + 1) % 4), ss=self.out),
                   self.net.copy(self.e.at[far, :, pl.ds(w, w)], self.tb, self.dev(f, (s + 3) % 4), ss=self.out))

    def step4(self):
        f, s, w = self.f, self.s, self.wide
        self.c4 = []
        for i, (d, got, dst) in enumerate(((1, self.ta, self.tp), (3, self.tb, self.tm))):
            self.c3[i].wait_recv()
            at = self.e.at[(s + d) % 4, :, pl.ds(i * w, w)]
            at[...] = (at[...].astype(jnp.float32) + got[...].astype(jnp.float32)).astype(self.kind)
            self.c4.append(self.net.copy(self.e.at[(s + d) % 4], dst, self.dev(f, (s + d) % 4), ss=self.out))

    def step5(self):
        for x in self.c4:
            x.wait_recv()
        total = self.e[self.s].astype(jnp.float32) + self.tp[...].astype(jnp.float32)
        return total + self.tm[...].astype(jnp.float32)


def route_scratch(rows, ch, kind):
    bf = jnp.bfloat16
    return [pltpu.VMEM((4, rows, ch // 2), bf), pltpu.VMEM((4, rows, ch // 2), bf),
            pltpu.VMEM((4, rows, ch), bf), pltpu.VMEM((4, rows, ch), bf), pltpu.VMEM((4, rows, ch), kind),
            pltpu.VMEM((rows, ch // 2), kind), pltpu.VMEM((rows, ch // 2), kind),
            pltpu.VMEM((rows, ch), kind), pltpu.VMEM((rows, ch), kind)]


class Stream:
    def __init__(self, net, buf, slots):
        self.net, self.out = net, net.new_send()
        self.blocks = 36 if slots[4].dtype == jnp.float32 else 30
        self.routes = [Route(net, buf, 0, True, slots[:9], self.out), Route(net, buf, 1, False, slots[9:], self.out)]

    def drain(self, flat):
        self.net.wait_send(flat.at[pl.ds(0, self.blocks)], self.out)

    def run(self, name):
        return [getattr(r, name)() for r in self.routes]


class Ring:
    def __init__(self, net, own, everyone):
        self.net, self.own, self.all = net, own, everyone
        t = lax.axis_index("tp")
        self.t = [t, (t + 3) % 4, (t + 1) % 4, (t + 2) % 4]
        self.onward = []

    def start(self):
        t = self.t
        self.up, self.down = [], []
        for j in range(4):
            self.up.append(self.copy(self.own.at[j], self.all.at[t[0], j], t[2]))
            i = (j + 2) % 4
            self.down.append(self.copy(self.own.at[i], self.all.at[t[0], i], t[1]))

    def copy(self, src, dst, tp):
        return self.net.copy(src, dst, lax.axis_index("kv"), tp)

    def pass_on(self, j):
        self.up[j].wait_recv()
        at = self.all.at[self.t[1], j]
        self.onward.append(self.copy(at, at, self.t[2]))
        self.down[j].wait_recv()
        at = self.all.at[self.t[2], j + 2]
        self.onward.append(self.copy(at, at, self.t[1]))

    def near(self):
        for c in self.up[2:] + self.down[2:]:
            c.wait_recv()

    def far(self):
        for c in self.onward:
            c.wait_recv()


def whole_kernel(chosen_ref, sums_ref, q_hbm, k_hbm, v_hbm, o_hbm, do_hbm, x_hbm,
                 dq_hbm, dk_hbm, dv_hbm, dw_ref, xall_hbm,
                 qb, kb, vb, ob, dob, dqt, dkb, dvb, dqb, delta_ref,
                 need, names, lse_ref, pick_ref, square, codes, codes_s, tab, pka, pva, pkb, pvb, gk, gv, part,
                 info, spots, info_s, spots_s, to_s, rka, rva, rkb, rvb, ws, wr, wb, *rest):
    kas, vas, kbs, vbs, wslots = (rest[i * 18:i * 18 + 18] for i in range(5))
    send, recv, local = rest[90:]
    z, y, c = place()
    me = lax.axis_index("kv")
    net, disk = Net(send, recv), Disk(local)
    loads = [disk.copy(a, b) for a, b in
             ((k_hbm, kb), (v_hbm, vb), (q_hbm, qb), (do_hbm, dob), (o_hbm, ob))]
    partner = kv_of(z, y, 1 - c)
    peers = [(me + d) % 32 for d in range(1, 32)]
    x = Ring(net, x_hbm, xall_hbm)
    greet(peers, x.t[1:3])
    seqs, n, ch = qb.shape
    half = n // 2

    def six(ref):
        return ref.reshape(2, 4, 4, CAP, BLK, ch // 2)

    blocks = n // BLK
    wide = ch // 2
    slots = 32 * CAP
    room = 18

    for t in range(seqs):
        v = chosen_ref[t]
        there = v >> 3
        codes[t, :, :12] = jnp.where((v >= 0) & (there != me), there * 128 + t * blocks + (v & 7), -1)
    to_codes = disk.copy(codes, codes_s)
    lse_ref[...] = sums_ref[...] * LOG2E
    rep_rows = lax.broadcasted_iota(jnp.int32, (128, n), 0)
    rep_cols = lax.broadcasted_iota(jnp.int32, (128, n), 1)
    stretch = jnp.where(rep_rows == rep_cols // BLK, 1.0, 0.0).astype(jnp.bfloat16)
    for t in range(seqs):
        square[...] = jnp.full((128, 128), -1.0, jnp.float32)
        square[:8, :12] = chosen_ref[t].astype(jnp.float32)
        pick_ref[t] = mm(square[...].astype(jnp.bfloat16), stretch, TN)[:16]
    flat = (lax.broadcasted_iota(jnp.int32, (32, 128), 0) * 128 +
            lax.broadcasted_iota(jnp.int32, (32, 128), 1))
    to_codes.wait()

    def mark(i, seen):
        for j in range(12):
            seen = jnp.where(flat == codes_s[i // 8, i % 8, j], 1, seen)
        return seen

    seen = lax.fori_loop(0, 32, mark, jnp.zeros((32, 128), jnp.int32))
    for i in range(32):
        need[i] = seen[i:i + 1]
    pl.semaphore_wait(pltpu.get_barrier_semaphore(), len(peers) + 2)
    told, heard = net.new_send(), net.new_recv()
    for d in range(1, 32):
        to = (me + d) % 32
        net.copy(need.at[to], names.at[me], to, ss=told, rs=heard)
    names[me] = jnp.zeros((1, 128), jnp.int32)
    x.start()
    for l in loads:
        l.wait()

    def hit_row(s, block):
        return jnp.max(jnp.where(pick_ref[s] == jnp.asarray(block, jnp.float32), 1.0, 0.0), axis=0, keepdims=True)

    def unit(u, _):
        s = u // 2
        hits = [hit_row(s, me * blocks + j) for j in range(blocks)]
        for g in range(2):
            h = (u % 2) * 2 + g
            hs = pl.ds(pl.multiple_of(h * DH, DH), DH)
            hr = pl.ds(h, 1)
            q = qb[s, :, hs]
            do = dob[s, :, hs]
            prod = do.astype(jnp.float32) * ob[s, :, :, hs].reshape(n, DH).astype(jnp.float32)
            delta = jnp.sum(prod.T, axis=0, keepdims=True)
            delta_ref[s, hr, :] = delta
            lse = lse_ref[s, hr, :]
            parts = []
            for t in range(2):
                lo = t * half
                here = slice(lo // BLK, (lo + half) // BLK)
                k = kb[s, here, :, hs].reshape(half, DH)
                v = vb[s, here, :, hs].reshape(half, DH)
                qc, doc = q[lo:], do[lo:]
                w = n - lo
                sc = mm(k, qc, NT)
                row = lax.broadcasted_iota(jnp.int32, (half, w), 0)
                col = lax.broadcasted_iota(jnp.int32, (half, w), 1)
                bias = jnp.concatenate(
                    [jnp.broadcast_to(jnp.where(hits[j] > 0.5, lse, BIG)[:, lo:], (BLK, w))
                     for j in range(lo // BLK, (lo + half) // BLK)], axis=0)
                p = jnp.exp2(jnp.where(row <= col, sc * (ROOT * LOG2E) - bias, -BIG))
                dp = mm(v, doc, NT)
                ds = (p * (dp - delta[:, lo:])).astype(jnp.bfloat16)
                dvb[s, here, :, hs] = mm(p.astype(jnp.bfloat16), doc, NN).astype(jnp.bfloat16).reshape(-1, BLK, DH)
                dkb[s, here, :, hs] = (mm(ds, qc, NN) * ROOT).astype(jnp.bfloat16).reshape(-1, BLK, DH)
                parts.append(mm(k, ds, TN))
            dqt[s, hs, :half] = parts[0][:, :half]
            dqt[s, hs, half:] = parts[0][:, half:] + parts[1]
        return 0

    def units(a, b):
        lax.fori_loop(a, b, unit, 0)

    units(0, 1)
    net.wait_recv(names.at[pl.ds(0, 31)], heard)
    need1 = jnp.broadcast_to(jnp.max(names[...], axis=0), (8, 128))
    info[...] = need1
    disk.copy(info, info_s).wait()

    def first_two(i, state):
        seen, s0, s1 = state
        here = info_s[0, i]
        s0 = jnp.where((here == 1) & (seen == 0), i, s0)
        s1 = jnp.where((here == 1) & (seen == 1), i, s1)
        return seen + here, s0, s1

    minus = jnp.int32(-1)
    _, served0, served1 = lax.fori_loop(0, seqs * blocks, first_two, (jnp.int32(0), minus, minus))
    served = (served0, served1)
    lane8 = lax.broadcasted_iota(jnp.int32, (8, 128), 1)
    tab[c, z, y] = jnp.where(lane8 == 0, served0, jnp.where(lane8 == 1, served1, minus))
    tys = [net.copy(tab.at[c, z, y], tab.at[c, z, y], kv_of(z, (y + d) % 4, c)) for d in range(1, 4)]

    def rows_of(ref):
        out = []
        for b in served:
            b = jnp.clip(b, 0, seqs * blocks - 1)
            out.append(ref[b // blocks, b % blocks])
        return out

    for b, (pick_k, pick_v) in enumerate(zip(rows_of(kb), rows_of(vb))):
        at = (c * 16 + z * 4 + y) * CAP + b
        pka[at] = pick_k[:, :wide]
        pva[at] = pick_v[:, :wide]
        pkb[at] = pick_k[:, wide:]
        pvb[at] = pick_v[:, wide:]

    ga = [Gather(net, six(pka), True), Gather(net, six(pva), False)]
    gb = [Gather(net, six(pkb), True), Gather(net, six(pvb), False)]

    def each(gs, name, *j):
        for g in gs:
            getattr(g, name)(*j)

    each(ga, "phase0")
    units(1, 3)
    for a in tys:
        a.wait_recv()
    tzs = [net.copy(tab.at[c, z], tab.at[c, z], kv_of((z + d) % 4, y, c)) for d in range(1, 4)]
    each(ga, "phase1")
    units(3, 5)
    each(ga, "phase2")
    each(gb, "phase0")
    for a in tzs:
        a.wait_recv()
    tside = net.copy(tab.at[c], tab.at[c], partner)
    units(5, 7)
    each(ga, "phase3", 0)
    each(ga, "phase3", 1)
    each(gb, "phase1")
    units(7, 8)
    own_x = disk.copy(x_hbm, kb)
    tside.wait_recv()
    for i in range(32):
        spots[i:i + 1] = tab[i // 16, i // 4 % 4, i % 4, 0:1]
    disk.copy(spots, spots_s).wait()

    def owner_of(p):
        o = p // CAP
        return o, o % 16 * 2 + o // 16

    def tally(p, sums):
        o, kvi = owner_of(p)
        v = spots_s[o, p % CAP]
        live = (v >= 0) & (kvi < me)
        return tuple(t + jnp.where(live & (v // blocks == s), 1, 0) for s, t in enumerate(sums))

    zero = jnp.int32(0)
    sums = lax.fori_loop(0, slots, tally, (zero,) * 4)
    chunks = [(t + 3) // 4 for t in sums]
    base = [zero]
    for s in range(3):
        base.append(base[-1] + chunks[s])

    def arrange(p, state):
        heads_at, l_slot, l_id = state
        o, kvi = owner_of(p)
        v = spots_s[o, p % CAP]
        live = (v >= 0) & (kvi < me)
        to = jnp.int32(4 * room)
        now = []
        for s, t in enumerate(heads_at):
            hit = live & (v // blocks == s)
            to = jnp.where(hit, t, to)
            now.append(t + jnp.where(hit, 1, 0))
        to_s[0, p] = to
        here = lane8 == to
        return tuple(now), jnp.where(here, p, l_slot), jnp.where(here, kvi * blocks + v % blocks, l_id)

    blank = jnp.zeros((8, 128), jnp.int32)
    _, l_slot, l_id = lax.fori_loop(
        0, slots, arrange, (tuple(4 * b for b in base), blank, blank - 5))
    row8 = lax.broadcasted_iota(jnp.int32, (8, 128), 0)
    info[...] = jnp.where(row8 == 0, l_slot, l_id)
    to_info = disk.copy(info, info_s)
    gk[4 * room] = jnp.zeros(gk.shape[1:], gk.dtype)
    gv[4 * room] = jnp.zeros(gv.shape[1:], gv.dtype)
    to_info.wait()
    count_me = jnp.where(me == 0, 0, (2 * me + 12) // 4)

    def seq_of(i):
        return sum(jnp.where(i >= base[s], 1, 0) for s in range(1, 4))

    each(ga, "phase3", 2)
    each(ga, "phase3", 3)
    each(gb, "phase2")
    for j in range(4):
        each(ga, "phase4", j)
    each(ga, "phase5")

    def attend(second):
        pk, pv = (pkb, pvb) if second else (pka, pva)

        def chunk(i, _):
            s = seq_of(i)
            keep = jnp.where((s == seq_of(i - 1)) & (i > 0), 1, 0)
            keep = jnp.broadcast_to(keep, (1, n)) == 1
            who = [(jnp.clip(info_s[0, 4 * i + e], 0, slots - 1), info_s[1, 4 * i + e]) for e in range(4)]
            hits = [hit_row(s, b) for _, b in who]
            for g in range(2):
                h = 2 * second + g
                gs = slice(g * DH, (g + 1) * DH)
                hs = slice(h * DH, (h + 1) * DH)
                q = qb[s, :, hs]
                do = dob[s, :, hs]
                k = jnp.concatenate([pk[o, :, gs] for o, _ in who], axis=0)
                v = jnp.concatenate([pv[o, :, gs] for o, _ in who], axis=0)
                lse = lse_ref[s, h:h + 1, :]
                st = mm(k, q, NT)
                bias = jnp.concatenate(
                    [jnp.broadcast_to(jnp.where(b > 0.5, lse, BIG), (BLK, n)) for b in hits], axis=0)
                p = jnp.exp2(st * (ROOT * LOG2E) - bias)
                dp = mm(v, do, NT)
                ds = (p * (dp - delta_ref[s, h:h + 1, :])).astype(jnp.bfloat16)
                dv = mm(p.astype(jnp.bfloat16), do, NN).astype(jnp.bfloat16)
                dk = (mm(ds, q, NN) * ROOT).astype(jnp.bfloat16)
                for e in range(4):
                    gv[4 * i + e, :, gs] = dv[e * BLK:(e + 1) * BLK]
                    gk[4 * i + e, :, gs] = dk[e * BLK:(e + 1) * BLK]
                old = part[2 * jnp.maximum(i - 1, 0) + g]
                part[2 * i + g] = jnp.where(keep, old, 0.0) + mm(k, ds, TN)
            return 0

        return lambda a, b: lax.fori_loop(jnp.minimum(a, count_me), jnp.minimum(b, count_me), chunk, 0)

    def settle(second):
        pk, pv = (pkb, pvb) if second else (pka, pva)

        def move(o, _):
            for b in range(CAP):
                to = jnp.clip(to_s[0, o * CAP + b], 0, 4 * room)
                pk[o * CAP + b] = gk[to]
                pv[o * CAP + b] = gv[to]
            return 0

        lax.fori_loop(0, 32, move, 0)

    def queries(second):
        for s in range(seqs):
            end = jnp.clip(base[s] + chunks[s] - 1, 0, room - 1)
            for g in range(2):
                h = 2 * second + g
                hs = slice(h * DH, (h + 1) * DH)
                more = jnp.where(jnp.broadcast_to(chunks[s], (1, n)) > 0, part[2 * end + g], 0.0)
                dqb[s, :, :, hs] = ((dqt[s, hs, :] + more).T * ROOT).astype(jnp.bfloat16).reshape(-1, BLK, DH)

    def side(buf, into):
        return net.copy(six(buf).at[1 - c], into, partner)

    def fold(buf, into, copy):
        copy.wait_recv()

        def add(i, _):
            at = c * 32 + i
            a = buf[at].astype(jnp.float32)
            buf[at] = (a + into[i // 8, i // 2 % 4, i % 2].astype(jnp.float32)).astype(jnp.bfloat16)
            return 0

        lax.fori_loop(0, 32, add, 0)

    first_half = attend(0)
    each(gb, "phase3", 0)
    first_half(0, 2)
    each(gb, "phase3", 1)
    first_half(2, 4)
    each(gb, "phase3", 2)
    first_half(4, 6)
    each(gb, "phase3", 3)
    first_half(6, 9)
    for j in range(2):
        each(gb, "phase4", j)
    first_half(9, 12)
    for j in range(2, 4):
        each(gb, "phase4", j)
    x.pass_on(0)
    first_half(12, room)
    each(gb, "phase5")
    ga[0].drain(pka)
    ga[1].drain(pva)
    settle(0)
    side_va = side(pva, rva)
    side_ka = side(pka, rka)
    queries(0)
    va = Stream(net, six(pva).at[c], vas)
    ka = Stream(net, six(pka).at[c], kas)
    second_half = attend(1)
    fold(pva, rva, side_va)
    va.run("step1")
    second_half(0, 2)
    fold(pka, rka, side_ka)
    ka.run("step1")
    second_half(2, 6)
    va.run("step2")
    x.pass_on(1)
    second_half(6, 10)
    ka.run("step2")
    second_half(10, 14)
    va.run("step3")
    second_half(14, room)
    gb[0].drain(pkb)
    gb[1].drain(pvb)
    settle(1)
    side_vb = side(pvb, rvb)
    side_kb = side(pkb, rkb)
    va.run("step4")
    ka.run("step3")
    queries(1)
    dq_out = disk.copy(dqb, dq_hbm)
    vsb = Stream(net, six(pvb).at[c], vbs)
    ksb = Stream(net, six(pkb).at[c], kbs)
    fold(pvb, rvb, side_vb)
    vsb.run("step1")
    ka.run("step4")
    fold(pkb, rkb, side_kb)

    x.near()
    load_x = [own_x, disk.copy(xall_hbm.at[x.t[1]], vb), disk.copy(xall_hbm.at[x.t[2]], ob)]
    bufs = [kb, vb, ob, dqb]

    def product(i):
        load_x[i].wait()

        def step(s, _):
            r = mm(bufs[i][s].reshape(n, ch), dvb[s].reshape(n, ch), TN)
            for j in range(4):
                at = x.t[i] * 4 + j
                part[at] = part[at] + r[j * 128:(j + 1) * 128]
            return 0

        r = mm(bufs[i][0].reshape(n, ch), dvb[0].reshape(n, ch), TN)
        for j in range(4):
            part[x.t[i] * 4 + j] = r[j * 128:(j + 1) * 128]
        lax.fori_loop(1, seqs, step, 0)

    product(0)
    vsb.run("step2")
    ksb.run("step1")
    fva = va.run("step5")
    product(1)
    fka = ka.run("step5")
    vsb.run("step3")
    product(2)
    vsb.run("step4")
    ksb.run("step2")
    x.far()
    dq_out.wait()
    load_x.append(disk.copy(xall_hbm.at[x.t[3]], dqb))
    product(3)
    old = jnp.concatenate(rows_of(dvb), axis=0).astype(jnp.float32)
    xs = [jnp.concatenate(rows_of(b), axis=0) for b in bufs]
    fvb = vsb.run("step5")

    def joined(a, b):
        return jnp.concatenate([jnp.concatenate(a, axis=0), jnp.concatenate(b, axis=0)], axis=1)

    extra_v = joined(fva, fvb)
    diff = ((old + extra_v).astype(jnp.bfloat16).astype(jnp.float32) - old).astype(jnp.bfloat16)
    mine, other = pl.multiple_of(c * BLK, BLK), pl.multiple_of((1 - c) * BLK, BLK)
    for i in range(4):
        r = mm(xs[i], diff, TN)
        for j in range(4):
            at = x.t[i] * 4 + j
            part[at] = part[at] + r[j * 128:(j + 1) * 128]
            ws[at] = part[at, pl.ds(other, BLK)].astype(jnp.bfloat16)
    side_w = net.copy(ws, wr, partner)
    ksb.run("step3")
    side_w.wait_recv()
    for i in range(16):
        own = part[i, pl.ds(mine, BLK)]
        wb[i // 4, i % 4] = (own + wr[i].astype(jnp.float32)).astype(jnp.bfloat16).reshape(2, BLK // 2, ch)
    w = Stream(net, wb, wslots)
    w.run("step1")
    ksb.run("step4")

    def finish(local_ref, extra):
        def add(i, _):
            at = (i // blocks, i % blocks)
            more = jnp.where(served0 == i, extra[:BLK], 0.0) + jnp.where(served1 == i, extra[BLK:], 0.0)
            local_ref[at] = (local_ref[at].astype(jnp.float32) + more).astype(jnp.bfloat16)
            return 0

        lax.fori_loop(0, seqs * blocks, add, 0)

    w.run("step2")
    finish(dvb, extra_v)
    disk.keep(dvb, dv_hbm)
    fkb = ksb.run("step5")
    w.run("step3")
    finish(dkb, joined(fka, fkb))
    disk.keep(dkb, dk_hbm)
    w.run("step4")
    top, low = w.run("step5")
    dw_ref[:BLK // 2] = top
    dw_ref[BLK // 2:] = low
    for st, ref in ((va, pva), (ka, pva), (vsb, pva), (ksb, pva), (w, pva)):
        st.drain(ref)
    net.wait_send(names.at[pl.ds(0, 31)], told)
    net.finish()
    disk.finish()
    assert net.n <= RECVS and net.ns <= SENDS, (net.n, net.ns)
    assert disk.n <= 16, disk.n


def fused(chosen, sums, q, k, v, o, do, x):
    seqs, n, ch = q.shape
    blk = k.shape
    heads = ch // DH
    bf, f32, i32 = jnp.bfloat16, jnp.float32, jnp.int32
    wide = ch // 2
    whole = pl.BlockSpec(memory_space=pltpu.VMEM)
    hbm = pl.BlockSpec(memory_space=pl.ANY)
    V = pltpu.VMEM
    return pl.pallas_call(
        whole_kernel,
        in_specs=[whole] * 2 + [hbm] * 6,
        out_specs=[hbm] * 3 + [whole, hbm],
        out_shape=[
            jax.ShapeDtypeStruct(blk, bf),
            jax.ShapeDtypeStruct(blk, bf),
            jax.ShapeDtypeStruct(blk, bf),
            jax.ShapeDtypeStruct((BLK, ch), f32),
            jax.ShapeDtypeStruct((4,) + x.shape, bf),
        ],
        scratch_shapes=[V(q.shape, bf)] + [V(blk, bf)] * 3 + [V(q.shape, bf), V((seqs, ch, n), f32)] + [V(blk, bf)] * 3 + [
            V((seqs, heads, n), f32),
            V((32, 1, 128), i32), V((32, 1, 128), i32), V((seqs, heads, n), f32), V((seqs, 16, n), f32),
            V((128, 128), f32), V((4, 8, 128), i32), pltpu.SMEM((4, 8, 128), i32), V((2, 4, 4, 8, 128), i32),
            V((64, BLK, wide), bf), V((64, BLK, wide), bf), V((64, BLK, wide), bf), V((64, BLK, wide), bf),
            V((73, BLK, wide), bf), V((73, BLK, wide), bf), V((36, DH, n), f32),
            V((8, 128), i32), V((32, 128), i32),
            pltpu.SMEM((8, 128), i32), pltpu.SMEM((32, 128), i32), pltpu.SMEM((8, 128), i32),
        ] + [V((4, 4, CAP, BLK, wide), bf)] * 4 + [
            V((16, BLK, ch), bf), V((16, BLK, ch), bf), V((4, 4, 2, BLK // 2, ch), bf),
        ] + (route_scratch(BLK, wide, bf) * 2 + route_scratch(BLK, wide, f32) * 2) * 2
        + route_scratch(BLK // 2, ch, f32) * 2 + [
            pltpu.SemaphoreType.DMA((SENDS,)), pltpu.SemaphoreType.DMA((RECVS,)), pltpu.SemaphoreType.DMA((16,)),
        ],
        compiler_params=pltpu.CompilerParams(
            vmem_limit_bytes=67043328, collective_id=0, has_side_effects=True),
        cost_estimate=pl.CostEstimate(flops=20_000_000_000, bytes_accessed=30 << 20, transcendentals=1 << 22),
        name="fused_backward",
    )(chosen, sums, q, k, v, o, do, x)


def hand_kernel(*refs):
    n = 4
    src, dst, buf, sems_in, sems_out = refs[:n], refs[n:2 * n], refs[2 * n:3 * n], refs[3 * n], refs[3 * n + 1]
    parts = [(a, p) for p in range(4) for a in range(n) if a < 3 or p == 0]

    def at(ref, a, p):
        return ref.at[p] if a < 3 else ref

    loads, stores = [], []
    for i, (a, p) in enumerate(parts):
        loads.append(pltpu.make_async_copy(at(src[a], a, p), at(buf[a], a, p), sems_in.at[i]))
        loads[-1].start()
    for i, (a, p) in enumerate(parts):
        loads[i].wait()
        stores.append(pltpu.make_async_copy(at(buf[a], a, p), at(dst[a], a, p), sems_out.at[i]))
        stores[-1].start()
    for c in stores:
        c.wait()


def hand_over(*arrays):
    hbm = pl.BlockSpec(memory_space=pl.ANY)
    return pl.pallas_call(
        hand_kernel,
        in_specs=[hbm] * 4,
        out_specs=[hbm] * 4,
        out_shape=[jax.ShapeDtypeStruct(a.shape, a.dtype) for a in arrays],
        scratch_shapes=[pltpu.VMEM(a.shape, a.dtype) for a in arrays] + [
            pltpu.SemaphoreType.DMA((13,)), pltpu.SemaphoreType.DMA((13,))],
        compiler_params=pltpu.CompilerParams(vmem_limit_bytes=60 * 1024 * 1024),
        name="hand_over",
    )(*arrays)


def body(layer_input, queries, keys, values, outputs, d_out, log_sums, chosen):
    seqs, n, ch = queries.shape
    blocks = n // BLK
    me = lax.axis_index("kv")
    def cut(a):
        return a.reshape(seqs, blocks, BLK, ch)

    dq, dk, dv, dw, _ = fused(chosen, jnp.swapaxes(log_sums, 1, 2), queries, cut(keys), cut(values),
                              cut(outputs), d_out, cut(layer_input))
    dq, dk, dv, dw = hand_over(dq, dk, dv, dw)
    return dq.reshape(queries.shape), dk.reshape(queries.shape), dv.reshape(queries.shape), dw


def solution(mesh):
    spec = P(None, "kv", "tp")
    return jax.shard_map(
        body,
        mesh=mesh,
        in_specs=(spec,) * 7 + (P(None, "kv", None),),
        out_specs=(spec, spec, spec, P("kv", "tp")),
        check_vma=False,
    )
```
